256 devices in a mesh: grp: 4 (over y, x), ep: 64 (over z, core).
Axes of the slice: x: 2, y: 2, z: 32, core: 2. Of those that a mesh axis runs over, the one named last changes fastest.
The devices are a block of a 4x8x32 slice.
Arguments:
- tokens: bfloat16 [256, 2048], P(('grp', 'ep')), parts along dimension 0, may hold values from -6 to 6
- cache_latent: bfloat16 [256, 3072, 512], P(('grp', 'ep')), parts along dimension 0, may hold values from -6 to 6
- cache_rope: bfloat16 [256, 32, 3072], P(('grp', 'ep')), parts along dimension 0, may hold values from -1000 to 1000
- lengths: int32 [256], P(('grp', 'ep')), parts along dimension 0, may hold values from 384 to 3072, as said below
- w_query: bfloat16 [2048, 1536], P('ep'), may hold values from -0.125 to 0.125
- w_latent: bfloat16 [2048, 512], P('ep'), may hold values from -0.125 to 0.125
- w_rope: bfloat16 [2048, 32], P('ep'), may hold values from -0.125 to 0.125
- w_absorb: bfloat16 [512, 1024], replicated, may hold values from -0.25 to 0.25
- w_value: bfloat16 [512, 1024], replicated, may hold values from -0.25 to 0.25
- w_output: bfloat16 [1024, 2048], P('ep'), may hold values from -0.1875 to 0.1875
- gain_attn: float32 [2048], replicated, may hold values from 0.1 to 1.9
- gain_latent: float32 [512], replicated, may hold values from 0.1 to 1.9
- gain_moe: float32 [2048], replicated, may hold values from 0.1 to 1.9
- routes: int32 [256, 2], P(('grp', 'ep')), parts along dimension 0, may hold values from 0 to 63, all different within a row; in each aligned block of 64 rows (0 to 63, 64 to 127, ...) at most 4 rows name the same one
- route_scores: float32 [256, 2], P(('grp', 'ep')), parts along dimension 0, may hold values from 0.2 to 1
- w_gate: bfloat16 [64, 2048, 512], P('ep'), may hold values from -0.125 to 0.125
- w_up: bfloat16 [64, 2048, 512], P('ep'), may hold values from -0.125 to 0.125
- w_down: bfloat16 [64, 512, 2048], P('ep'), may hold values from -0.25 to 0.25
Outputs:
- mixed: bfloat16 [256, 2048], P(('grp', 'ep')), parts along dimension 0
- new_latent: bfloat16 [256, 512], P(('grp', 'ep')), parts along dimension 0
- new_rope: bfloat16 [256, 32], P(('grp', 'ep')), parts along dimension 0
The draws below stay inside these ranges and needn't reach their ends.
There are 4 independent parts, one for each index of `grp`. The reference program is written for one: setup_inputs(seed, part) draws one part's arguments, and reference() takes and returns one part's arrays. A program takes and returns all parts, laid end to end along the dimension named above; an argument that names none is the same for every part. Nothing has to cross between parts.
Inputs may be any that keep to these rules, and one draw needn't show every extreme that they name: `routes`: each row names 2 different experts; over one part's 64 tokens no expert is named by more than 4 rows, a bound that some block reaches. `lengths`: some sequence has all 3072 positions filled.
All inputs are finite; a program needn't handle non-finite values.
Results may differ from the reference program's by a relative error of at most 0.013.
Values may be sent and summed in bfloat16 or wider, within the bound.
A program may use at most 64 MiB of HBM per device.

```python
import math
import jax
import jax.numpy as jnp
import numpy as np
from jax import lax

D = 2048
HEADS = 16
NOPE = 64
ROPE = 32
VDIM = 64
LATENT = 512
FF = 512
TOPK = 2
CACHE = 3072
SEQS = 64
EXPERTS = 64
CAP = 4


def draw_cache_rope(key, part):
    k_base = jax.random.fold_in(jax.random.fold_in(key, 31), 0)
    base = jnp.clip(jax.random.normal(k_base, (SEQS, ROPE, CACHE), jnp.float32), -6.0, 6.0)
    return base.astype(jnp.bfloat16)


def draw_lengths(key, part):
    k_len, k_full = jax.random.split(jax.random.fold_in(key, 23))
    values = jax.random.randint(k_len, (SEQS,), CACHE // 8, CACHE + 1)
    chosen = jax.random.randint(k_full, (), 0, SEQS)
    values = jnp.where(jnp.arange(SEQS) == chosen, CACHE, values)
    return values.astype(jnp.int32)


def block_scale(own_key, extent, shards, low, top_value):
    def one(dim, shards_of):
        draws = jax.random.uniform(jax.random.fold_in(jax.random.fold_in(own_key, 6), dim), (shards_of,), jnp.float32, low / len(shards), top_value / len(shards))
        return jnp.repeat(jnp.exp(draws), extent[dim] // shards_of).reshape((-1,) + (1,) * (len(extent) - dim - 1))

    level = one(*shards[0])
    for cut in shards[1:]:
        level = level * one(*cut)
    return level


def assign_block(own_key, own, number, rows, number_of, top, most, lean):
    order = jax.random.permutation(own_key, number_of)
    crowded, ordinary = portions_of(number_of, rows * top, most, lean, True), portions_of(number_of, rows * top, most, lean, False)
    places = jnp.arange(number_of)

    def named(sizes, turn):
        used = int((sizes > 0).sum())
        fixed = max(1, used // 4)
        moved = fixed + (places - fixed + turn * (used - fixed)) % max(1, number_of - fixed)
        return jnp.zeros((number_of,), jnp.int32).at[order[jnp.where(places < fixed, places, moved)]].set(jnp.asarray(sizes, jnp.int32))

    sizes = jnp.where(number % 4 == 0, named(crowded, number // 4), named(ordinary, number - number // 4 - 1))
    mixed = jax.random.permutation(jax.random.fold_in(own, 3), number_of)
    donor, receiver = mixed[0:number_of // 2 * 2:2], mixed[1:number_of // 2 * 2:2]
    margin = jnp.minimum(sizes[donor] - 1, most - sizes[receiver]) // 2
    margin = jnp.where((donor == order[0]) | (receiver == order[0]) | (sizes[receiver] == 0), 0, jnp.maximum(margin, 0))
    moved = jax.random.randint(jax.random.fold_in(own, 4), (number_of // 2,), 0, 1 << 20) % (margin + 1)
    sizes = sizes.at[donor].add(-moved).at[receiver].add(moved)
    items = jnp.searchsorted(jnp.cumsum(sizes), jnp.arange(rows * top), side="right").astype(jnp.int32)
    table = items.reshape(top, rows).T
    table = table[jax.random.permutation(jax.random.fold_in(own, 1), rows)]
    turn = jax.random.randint(jax.random.fold_in(own, 2), (rows, 1), 0, top)
    return jnp.take_along_axis(table, (jnp.arange(top)[None, :] + turn) % top, axis=1)


def portions_of(number_of, total, bound, lean, full):
    portions = [(1 << 20) // math.isqrt(grade ** lean) + 1 for grade in range(1, number_of + 1)]
    largest = bound if full else min(bound, max(-(-total // number_of), total * portions[0] // sum(portions)))
    least = 1 if total - largest >= number_of - 1 else 0
    given, spare = [largest] + [least] * (number_of - 1), total - largest - least * (number_of - 1)
    while spare > 0:
        free = [i for i in range(1, number_of) if given[i] < largest] or [i for i in range(1, number_of) if given[i] < bound]
        whole, remaining = sum([portions[i] for i in free]), spare
        for i in free:
            extra = min(bound - given[i], max(1, remaining * portions[i] // whole), spare)
            given[i] = given[i] + extra
            spare = spare - extra
    return np.array(given)


def scatter_about(stream_key, shape, scale, reach, cuts=(), held_as=jnp.bfloat16):
    array = jax.random.normal(stream_key, shape, jnp.float32) * scale
    if len(cuts) > 0:
        array = block_scale(stream_key, shape, cuts, -0.22, 0.18) * array
    return jnp.clip(array, min=-reach, max=reach).astype(held_as)


def setup_inputs(seed: int = 0, part: int = 0) -> dict:
    streams_of = jax.random.split(jax.random.key(seed), 19)
    own_keys = jax.random.split(jax.random.fold_in(streams_of[18], part), 19)
    tokens = scatter_about(own_keys[0], (SEQS, D), 1.0, 6.0, ((0, 64),))
    cache_latent = scatter_about(own_keys[1], (SEQS, CACHE, LATENT), 1.0, 6.0, ((0, 64),))
    cache_rope = draw_cache_rope(jax.random.fold_in(jax.random.fold_in(streams_of[18], part), 71), part)
    lengths = draw_lengths(jax.random.fold_in(jax.random.fold_in(streams_of[18], part), 71), part)
    w_query = scatter_about(streams_of[4], (D, HEADS * (NOPE + ROPE)), D ** -0.5, 0.125, ((0, 64),))
    w_latent = scatter_about(streams_of[5], (D, LATENT), D ** -0.5, 0.125, ((0, 64),))
    w_rope = scatter_about(streams_of[6], (D, ROPE), D ** -0.5, 0.125, ((0, 64),))
    w_absorb = scatter_about(streams_of[7], (LATENT, HEADS * NOPE), LATENT ** -0.5, 0.25)
    w_value = scatter_about(streams_of[8], (LATENT, HEADS * VDIM), LATENT ** -0.5, 0.25)
    w_output = scatter_about(streams_of[9], (HEADS * VDIM, D), (HEADS * VDIM) ** -0.5, 0.1875, ((0, 64),))
    gain_attn = jnp.clip(1.0 + 0.18 * jax.random.normal(streams_of[10], (D,), jnp.float32), 0.1, 1.9)
    gain_latent = jnp.clip(1.0 + 0.18 * jax.random.normal(streams_of[11], (LATENT,), jnp.float32), 0.1, 1.9)
    gain_moe = jnp.clip(1.0 + 0.18 * jax.random.normal(streams_of[12], (D,), jnp.float32), 0.1, 1.9)
    routes_keys = jax.random.split(jax.random.fold_in(own_keys[13], 1), SEQS // SEQS)
    routes_turns = jax.random.permutation(jax.random.fold_in(own_keys[13], 3), SEQS // SEQS)
    routes = jax.vmap(lambda own, number: assign_block(jax.random.fold_in(own_keys[13], 2), own, number, SEQS, EXPERTS, TOPK, CAP, 2))(routes_keys, routes_turns).reshape((SEQS, TOPK))
    route_scores = jnp.clip(jnp.exp(math.log(1.0) - 1.609438 * jax.random.uniform(own_keys[14], (SEQS, TOPK), jnp.float32) ** block_scale(own_keys[14], (SEQS, TOPK), ((0, 64),), -0.2, 0.2)), 0.2, 1.0)
    w_gate = scatter_about(streams_of[15], (EXPERTS, D, FF), D ** -0.5, 0.125, ((0, 64),))
    w_up = scatter_about(streams_of[16], (EXPERTS, D, FF), D ** -0.5, 0.125, ((0, 64),))
    w_down = scatter_about(streams_of[17], (EXPERTS, FF, D), FF ** -0.5, 0.25, ((0, 64),))
    return {"tokens": tokens, "cache_latent": cache_latent, "cache_rope": cache_rope, "lengths": lengths, "w_query": w_query, "w_latent": w_latent, "w_rope": w_rope, "w_absorb": w_absorb, "w_value": w_value, "w_output": w_output, "gain_attn": gain_attn, "gain_latent": gain_latent, "gain_moe": gain_moe, "routes": routes, "route_scores": route_scores, "w_gate": w_gate, "w_up": w_up, "w_down": w_down}


EPS = 1e-06
THETA = 10000.0

def rms_scale(values, gain):
    return values * lax.rsqrt(lax.optimization_barrier(jnp.mean(values * values, axis=-1, keepdims=True)) + EPS) * gain.astype(jnp.float32)

def rope_tables(positions, width):
    inverse = THETA ** (-jnp.arange(0, width, 2).astype(jnp.float32) / width)
    angle = positions.astype(jnp.float32)[:, None] * inverse[None, :]
    return (jnp.cos(angle), jnp.sin(angle))

def apply_rope(values, cosine, sine):
    half = values.shape[-1] // 2
    first, second = (values[..., :half], values[..., half:])
    return jnp.concatenate([first * cosine - second * sine, second * cosine + first * sine], axis=-1)

def attend_one(items):
    q_abs, q_pe, lat_cache, rope_cache, ckv, kpe, length = items
    scale = (NOPE + ROPE) ** (-0.5)
    past = (jnp.einsum('hc,kc->hk', q_abs.astype(jnp.float32), lat_cache.astype(jnp.float32)) + jnp.einsum('hr,rk->hk', q_pe.astype(jnp.float32), rope_cache.astype(jnp.float32))) * scale
    fresh = (jnp.einsum('hc,c->h', q_abs.astype(jnp.float32), ckv.astype(jnp.float32)) + jnp.einsum('hr,r->h', q_pe.astype(jnp.float32), kpe.astype(jnp.float32))) * scale
    valid = jnp.arange(lat_cache.shape[0]).astype(jnp.int32)[None, :] < length
    top = jnp.maximum(lax.optimization_barrier(jnp.max(jnp.where(valid, past, -jnp.inf), axis=-1)), fresh)
    e_past = jnp.where(valid, jnp.exp(past - top[:, None]), 0.0)
    e_new = jnp.exp(fresh - top)
    total = lax.optimization_barrier(jnp.sum(e_past, axis=-1)) + e_new
    p_past = (e_past / total[:, None]).astype(jnp.bfloat16)
    p_new = (e_new / total).astype(jnp.bfloat16)
    out = jnp.einsum('hk,kc->hc', p_past.astype(jnp.float32), lat_cache.astype(jnp.float32)) + p_new.astype(jnp.float32)[:, None] * ckv.astype(jnp.float32)[None, :]
    return out.astype(jnp.bfloat16)

def reference(tokens, cache_latent, cache_rope, lengths, w_query, w_latent, w_rope, w_absorb, w_value, w_output, gain_attn, gain_latent, gain_moe, routes, route_scores, w_gate, w_up, w_down):
    count = tokens.shape[0]
    normed = rms_scale(tokens.astype(jnp.float32), gain_attn).astype(jnp.bfloat16)
    query = jnp.dot(normed, w_query, preferred_element_type=jnp.float32).astype(jnp.bfloat16)
    latent_raw = jnp.dot(normed, w_latent, preferred_element_type=jnp.float32).astype(jnp.bfloat16)
    rope_raw = jnp.dot(normed, w_rope, preferred_element_type=jnp.float32).astype(jnp.bfloat16)
    new_latent = rms_scale(latent_raw.astype(jnp.float32), gain_latent).astype(jnp.bfloat16)
    cosine, sine = rope_tables(lengths, ROPE)
    new_rope = apply_rope(rope_raw.astype(jnp.float32), cosine, sine).astype(jnp.bfloat16)
    heads_view = query.reshape(count, HEADS, NOPE + ROPE)
    q_nope = heads_view[:, :, :NOPE]
    q_pe = apply_rope(heads_view[:, :, NOPE:].astype(jnp.float32), cosine[:, None, :], sine[:, None, :]).astype(jnp.bfloat16)
    q_abs = jnp.einsum('shn,chn->shc', q_nope.astype(jnp.float32), w_absorb.reshape(LATENT, HEADS, NOPE).astype(jnp.float32)).astype(jnp.bfloat16)
    attended = lax.map(attend_one, (q_abs, q_pe, cache_latent, cache_rope, new_latent, new_rope, lengths))
    values = jnp.einsum('shc,chv->shv', attended.astype(jnp.float32), w_value.reshape(LATENT, HEADS, VDIM).astype(jnp.float32)).astype(jnp.bfloat16)
    attn_out = jnp.dot(values.reshape(count, HEADS * VDIM), w_output, preferred_element_type=jnp.float32)
    resid = (tokens.astype(jnp.float32) + attn_out).astype(jnp.bfloat16)
    moe_in = rms_scale(resid.astype(jnp.float32), gain_moe).astype(jnp.bfloat16)

    def expert_one(items):
        index, row = items
        gate = jnp.dot(row[None, :], w_gate[index], preferred_element_type=jnp.float32)
        upper = jnp.dot(row[None, :], w_up[index], preferred_element_type=jnp.float32)
        hidden = (jax.nn.silu(gate) * upper).astype(jnp.bfloat16)
        return jnp.dot(hidden, w_down[index], preferred_element_type=jnp.float32).astype(jnp.bfloat16)[0]
    flat_ids = routes.reshape(-1).astype(jnp.int32)
    flat_rows = jnp.repeat(moe_in, TOPK, axis=0)
    expert_out = lax.map(expert_one, (flat_ids, flat_rows)).reshape(count, TOPK, D)
    route_weight = route_scores / lax.optimization_barrier(jnp.sum(route_scores, axis=-1, keepdims=True))
    moe_sum = lax.optimization_barrier(jnp.sum(route_weight[:, :, None] * expert_out.astype(jnp.float32), axis=1))
    mixed = (resid.astype(jnp.float32) + moe_sum).astype(jnp.bfloat16)
    return (mixed, new_latent, new_rope)
```

```python
import functools

import jax
import jax.numpy as jnp
from jax import lax
from jax.experimental import pallas as pl
from jax.experimental.pallas import tpu as pltpu
from jax.sharding import PartitionSpec as P

HEADS = 16
NOPE = 64
ROPE = 32
VDIM = 64
LATENT = 512
EPS = 1e-06
THETA = 10000.0
MESH = pl.DeviceIdType.MESH
F32 = jnp.float32
BF16 = jnp.bfloat16


def rope_tables(positions, width):
    inverse = THETA ** (-jnp.arange(0, width, 2).astype(F32) / width)
    angle = positions.astype(F32)[:, None] * inverse[None, :]
    return (jnp.cos(angle), jnp.sin(angle))


def farthest_first(i, n):
    half = (i + 1) // 2
    return n // 2 + half * (1 - 2 * lax.rem(i, 2))


def rotate(x, cosine, sine):
    lanes = x.shape[-1]
    place = lax.rem(lax.broadcasted_iota(jnp.int32, x.shape, 1), ROPE)
    ahead = pltpu.roll(x, lanes - ROPE // 2, 1)
    behind = pltpu.roll(x, ROPE // 2, 1)
    return jnp.where(place < ROPE // 2, x * cosine - ahead * sine, x * cosine + behind * sine)


def dot(a, b):
    return jnp.dot(a, b, preferred_element_type=F32)


def dot_nt(a, b):
    return lax.dot_general(a, b, (((1,), (1,)), ((), ())), preferred_element_type=F32)


def kernel(
    nz,
    length_ref,
    tokens_hbm,
    cache_hbm,
    rope_hbm,
    wq_hbm,
    wl_hbm,
    wr_hbm,
    wa_hbm,
    wv_hbm,
    wo_hbm,
    gain_attn_hbm,
    gain_latent_hbm,
    gain_moe_hbm,
    cos_hbm,
    sin_hbm,
    wt_hbm,
    wg_hbm,
    wu_hbm,
    wd_hbm,
    mixed_ref,
    new_latent_ref,
    new_rope_ref,
    tokens_v,
    gain_attn_v,
    gain_latent_v,
    gain_moe_v,
    cos_v,
    sin_v,
    wt_v,
    cache_v,
    rope_v,
    wa_v,
    wv_v,
    wq_v,
    wl_v,
    wr_v,
    wo_v,
    wg_v,
    wu_v,
    wd_v,
    p1_send,
    p1_recv,
    wt_recv,
    p2_send,
    p2_recv,
    p3_send,
    p3_recv,
    x3,
    c4,
    p4_send,
    p4_recv,
    local_sem,
    send16,
    send32,
    sendw,
    p1_sem,
    wt_sem,
    p2_sem,
    p3_sem,
    p4_sem,
    w_send,
    w_recv,
    e_send,
    e_recv,
    right_send,
    right_recv,
    left_send,
    left_recv,
    part_send,
    part_recv,
):
    g = lax.axis_index("grp")
    e = lax.axis_index("ep")
    z = e // 2
    c = lax.rem(e, 2)
    m = z // 2
    p = lax.rem(z, 2)
    nm = nz // 2
    q_width = wq_hbm.shape[1]
    lat = wl_hbm.shape[1]
    ropes = wr_hbm.shape[1]
    fper = wq_hbm.shape[0]
    feats = 4 * fper
    d_model = tokens_hbm.shape[1]
    half = d_model // 2
    cache = cache_v.shape[0]

    def dev(zz, cc):
        return (g, zz * 2 + cc)

    beside = z + 1 - 2 * p
    right = lax.rem(z + 1, nz)
    left = lax.rem(z + nz - 1, nz)

    def remote(src, dst, send, recv, to):
        return pltpu.make_async_remote_copy(
            src_ref=src, dst_ref=dst, send_sem=send, recv_sem=recv, device_id=to, device_id_type=MESH
        )

    barrier = pltpu.get_barrier_semaphore()

    def greet(i, _):
        pl.semaphore_signal(barrier, inc=1, device_id=dev(lax.rem(z + i, nz), c), device_id_type=MESH)
        return 0

    lax.fori_loop(1, nz, greet, 0)
    pl.semaphore_signal(barrier, inc=1, device_id=dev(z, 1 - c), device_id_type=MESH)
    pl.semaphore_signal(barrier, inc=1, device_id=dev(beside, 1 - c), device_id_type=MESH)

    block = 2 * p + c
    rows = pl.ds(pl.multiple_of(block * fper, fper), fper)
    loads = [
        (tokens_hbm, tokens_v),
        (gain_attn_hbm, gain_attn_v),
        (wt_hbm, wt_v),
        (wq_hbm, wq_v.at[rows]),
        (wl_hbm, wl_v.at[rows]),
        (wr_hbm, wr_v.at[rows]),
        (gain_latent_hbm, gain_latent_v),
        (gain_moe_hbm, gain_moe_v),
        (cos_hbm, cos_v),
        (sin_hbm, sin_v),
        (wo_hbm, wo_v.at[e]),
        (wa_hbm, wa_v),
        (cache_hbm.at[0], cache_v),
        (rope_hbm.at[0], rope_v),
        (wv_hbm, wv_v),
        (wg_hbm.at[0], wg_v.at[c]),
        (wu_hbm.at[0], wu_v.at[c]),
        (wd_hbm.at[0], wd_v.at[c]),
    ]
    local = [pltpu.make_async_copy(a, b, local_sem.at[i]) for i, (a, b) in enumerate(loads)]
    for copy in local:
        copy.start()

    local[0].wait()
    local[1].wait()
    local[2].wait()
    tokens = tokens_v[...].astype(F32)
    normed = tokens * lax.rsqrt(jnp.mean(tokens * tokens, axis=-1, keepdims=True) + EPS) * gain_attn_v[...]
    normed = normed.astype(BF16).astype(F32)
    for i in range(nm):
        p1_send[i] = normed[:, i * feats : (i + 1) * feats]
    p1_recv[m] = p1_send[m]
    wt_recv[z] = wt_v[...]
    p2_send[...] = jnp.zeros_like(p2_send)

    pl.semaphore_wait(barrier, nz + 1)

    def p1_copy(to, slot, d):
        return remote(p1_send.at[to], p1_recv.at[slot], send16.at[d], p1_sem.at[slot], dev(2 * to + p, c))

    def p1_start(i, _):
        d = farthest_first(i, nm)
        p1_copy(lax.rem(m + d, nm), m, d).start()
        return 0

    lax.fori_loop(0, nm - 1, p1_start, 0)

    w_pairs = ((wq_hbm, wq_v), (wl_hbm, wl_v), (wr_hbm, wr_v))
    w_targets = (dev(beside, c), dev(beside, 1 - c), dev(z, 1 - c))

    def w_copies(slot, k):
        at = pl.ds(pl.multiple_of(slot * fper, fper), fper)
        return [
            remote(src, dst.at[at], w_send.at[3 * k + j], w_recv.at[3 * slot + j], w_targets[k])
            for j, (src, dst) in enumerate(w_pairs)
        ]

    for k in range(3):
        for copy in w_copies(block, k):
            copy.start()

    def to_part(src, zz):
        return remote(src, wo_v.at[2 * zz + c], part_send.at[zz], part_recv.at[zz], dev(z, 1 - c))

    def to_right(src, zz, s):
        return remote(src, wo_v.at[2 * zz + c], right_send.at[s], right_recv.at[s], dev(right, c))

    def to_left(src, zz, s):
        return remote(src, wo_v.at[2 * zz + c], left_send.at[s], left_recv.at[s], dev(left, c))

    to_right(wo_hbm, z, 0).start()
    to_left(wo_hbm, z, 0).start()
    to_part(wo_hbm, z).start()

    def from_left(s, forward):
        zz = lax.rem(z + nz - s, nz)
        mine = wo_v.at[2 * zz + c]
        to_right(mine, zz, s - 1).wait_recv()
        if forward:
            to_right(mine, zz, s).start()
        to_part(mine, zz).start()

    def from_right(s, forward):
        zz = lax.rem(z + s, nz)
        mine = wo_v.at[2 * zz + c]
        to_left(mine, zz, s - 1).wait_recv()
        if forward:
            to_left(mine, zz, s).start()
        to_part(mine, zz).start()

    def ring(first, last):
        def step(s, _):
            from_left(s, True)
            from_right(s, True)
            return 0

        lax.fori_loop(first, last + 1, step, 0)

    def wt_copy(to, slot, d):
        return remote(wt_v, wt_recv.at[slot], sendw.at[d], wt_sem.at[slot], dev(to, c))

    def wt_start(i, _):
        d = farthest_first(i, nz)
        wt_copy(lax.rem(z + d, nz), z, d).start()
        return 0

    lax.fori_loop(0, nz - 1, wt_start, 0)

    e_pairs = ((wg_hbm, wg_v), (wu_hbm, wu_v), (wd_hbm, wd_v))

    def e_copies(slot):
        return [
            remote(src.at[0], dst.at[slot], e_send.at[j], e_recv.at[j], dev(z, 1 - c))
            for j, (src, dst) in enumerate(e_pairs)
        ]

    for copy in e_copies(c):
        copy.start()

    ring(1, 3)

    for copy in local[3:6]:
        copy.wait()
    for k in range(1, 4):
        for copy in w_copies(lax.rem(block + k, 4), 0):
            copy.wait_recv()

    def p1_wait(i, _):
        d = farthest_first(i, nm)
        p1_copy(m, lax.rem(m + nm - d, nm), d).wait_recv()
        return 0

    lax.fori_loop(0, nm - 1, p1_wait, 0)

    def p1_sent(d, _):
        p1_copy(m, m, d).wait_send()
        return 0

    lax.fori_loop(1, nm, p1_sent, 0)

    x1 = p1_recv[:, 0, :].astype(BF16)
    part_q = dot(x1, wq_v[...])
    part_l = dot(x1, wl_v[...])
    part_r = dot(x1, wr_v[...])
    for i in range(nm):
        p2_send[i, :, 0:q_width] = part_q[i : i + 1, :]
        p2_send[i, :, q_width : q_width + lat] = part_l[i : i + 1, :]
        p2_send[i, :, q_width + lat : q_width + lat + ropes] = part_r[i : i + 1, :]

    def p2_copy(to, slot, d):
        return remote(p2_send.at[to], p2_recv.at[slot], send16.at[d], p2_sem.at[slot], dev(2 * to + p, c))

    def p2_start(i, _):
        d = farthest_first(i, nm)
        p2_copy(lax.rem(m + d, nm), m, d).start()
        return 0

    lax.fori_loop(0, nm - 1, p2_start, 0)

    ring(4, 8)

    def p2_wait(i, acc):
        d = nm - 1 - i
        src = lax.rem(m + nm - d, nm)
        p2_copy(m, src, d).wait_recv()
        return acc + p2_recv[src]

    summed = lax.fori_loop(0, nm - 1, p2_wait, p2_send[m])

    for copy in local[6:10]:
        copy.wait()
    query = summed[:, :q_width].astype(BF16).astype(F32)
    latent_raw = summed[:, q_width : q_width + lat].astype(BF16).astype(F32)
    rope_raw = summed[:, q_width + lat :].astype(BF16).astype(F32)
    new_latent = (
        latent_raw
        * lax.rsqrt(jnp.mean(latent_raw * latent_raw, axis=-1, keepdims=True) + EPS)
        * gain_latent_v[...]
    ).astype(BF16)
    cosine, sine = cos_v[...], sin_v[...]
    new_rope = rotate(rope_raw, cosine[:, : rope_raw.shape[1]], sine[:, : rope_raw.shape[1]]).astype(BF16)
    new_latent_ref[...] = new_latent
    new_rope_ref[...] = new_rope[:, :ropes]

    size = NOPE + ROPE
    q_nope = jnp.concatenate([query[:, h * size : h * size + NOPE] for h in range(HEADS)], axis=1)
    q_rope = jnp.concatenate([query[:, h * size + NOPE : (h + 1) * size] for h in range(HEADS)], axis=1)
    q_rope = rotate(q_rope, cosine, sine).astype(BF16).astype(F32)

    def by_head(row, width):
        shape = (HEADS, row.shape[1])
        own = lax.broadcasted_iota(jnp.int32, shape, 1) // width == lax.broadcasted_iota(jnp.int32, shape, 0)
        return jnp.where(own, jnp.broadcast_to(row, shape), 0.0)

    fold_shape = (HEADS * ROPE, ROPE)
    fold = (
        lax.rem(lax.broadcasted_iota(jnp.int32, fold_shape, 0), ROPE)
        == lax.broadcasted_iota(jnp.int32, fold_shape, 1)
    ).astype(F32).astype(BF16)
    q_pe = dot(by_head(q_rope, ROPE).astype(BF16), fold).astype(BF16)
    local[11].wait()
    q_abs = dot_nt(by_head(q_nope, NOPE).astype(BF16), wa_v[...]).astype(BF16)

    local[12].wait()
    local[13].wait()
    scale = (NOPE + ROPE) ** (-0.5)
    past = (dot_nt(q_abs, cache_v[...]) + dot(q_pe, rope_v[...])) * scale
    fresh = (
        jnp.sum(q_abs.astype(F32) * new_latent.astype(F32), axis=-1, keepdims=True)
        + jnp.sum(q_pe.astype(F32) * new_rope[:, :ropes].astype(F32), axis=-1, keepdims=True)
    ) * scale
    valid = lax.broadcasted_iota(jnp.int32, past.shape, 1) < length_ref[0]
    top = jnp.maximum(jnp.max(jnp.where(valid, past, -jnp.inf), axis=-1, keepdims=True), fresh)
    e_past = jnp.where(valid, jnp.exp(past - top), 0.0)
    e_new = jnp.exp(fresh - top)
    total = jnp.sum(e_past, axis=-1, keepdims=True) + e_new
    p_past = (e_past / total).astype(BF16)
    p_new = (e_new / total).astype(BF16).astype(F32)
    attended = (dot(p_past, cache_v[...]) + p_new * new_latent.astype(F32)).astype(BF16)
    local[14].wait()
    crossed = dot(attended, wv_v[...])
    own_head = (
        lax.broadcasted_iota(jnp.int32, crossed.shape, 1) // VDIM
        == lax.broadcasted_iota(jnp.int32, crossed.shape, 0)
    )
    values = jnp.sum(jnp.where(own_head, crossed, 0.0), axis=0, keepdims=True).astype(BF16)

    ring(9, nm - 2)
    from_left(nm - 1, True)
    from_right(nm - 1, False)
    from_left(nm, False)
    local[10].wait()

    def part_wait(zz, _):
        remote(
            wo_v.at[2 * zz + 1 - c], wo_v.at[2 * zz + 1 - c], part_send.at[zz], part_recv.at[zz], dev(z, 1 - c)
        ).wait_recv()
        return 0

    lax.fori_loop(0, nz, part_wait, 0)

    attn_out = dot(values, wo_v[...].reshape(-1, d_model))
    resid = (tokens + attn_out).astype(BF16).astype(F32)
    moe_in = resid * lax.rsqrt(jnp.mean(resid * resid, axis=-1, keepdims=True) + EPS) * gain_moe_v[...]
    moe_in = moe_in.astype(BF16).astype(F32)
    p3_send[...] = jnp.concatenate([moe_in[:, :half], moe_in[:, half:]], axis=0).astype(BF16)

    def p3_copy(to, slot, d):
        return remote(p3_send, p3_recv.at[slot], send32.at[d], p3_sem.at[slot], dev(to, c))

    def p3_start(i, _):
        d = farthest_first(i, nz)
        p3_copy(lax.rem(z + d, nz), z, d).start()
        return 0

    lax.fori_loop(0, nz - 1, p3_start, 0)
    x3[pl.ds(z, 1), :] = moe_in

    for copy in local[15:18]:
        copy.wait()
    for copy in e_copies(1 - c):
        copy.wait_recv()

    def wt_wait(i, _):
        d = i + 1
        wt_copy(z, lax.rem(z + nz - d, nz), d).wait()
        return 0

    lax.fori_loop(0, nz - 1, wt_wait, 0)

    def p3_wait(i, _):
        near = i // 2 + 1
        src = lax.rem(z + nz + near * (1 - 2 * lax.rem(i, 2)), nz)
        p3_copy(z, src, 0).wait_recv()
        row = p3_recv[src].astype(F32)
        x3[pl.ds(src, 1), 0:half] = row[0:1]
        x3[pl.ds(src, 1), half:d_model] = row[1:2]
        return 0

    lax.fori_loop(0, nz - 1, p3_wait, 0)

    def p3_sent(d, _):
        p3_copy(z, z, d).wait_send()
        return 0

    lax.fori_loop(1, nz, p3_sent, 0)

    rows3 = x3[...].astype(BF16)
    shares = wt_recv[:, 0, :]
    expert = lax.broadcasted_iota(jnp.int32, shares.shape, 1)
    outs = []
    for s in range(2):
        share = jnp.sum(jnp.where(expert == 2 * z + s, shares, 0.0), axis=1, keepdims=True)
        gate = dot(rows3, wg_v[s])
        upper = dot(rows3, wu_v[s])
        hidden = (jax.nn.silu(gate) * upper).astype(BF16)
        result = dot(hidden, wd_v[s]).astype(BF16).astype(F32)
        outs.append(share * result)
    c4[...] = outs[0] + outs[1]

    def p4_copy(to, slot, d):
        return remote(p4_send.at[to], p4_recv.at[slot], send32.at[d], p4_sem.at[slot], dev(to, c))

    def p4_start(i, _):
        d = farthest_first(i, nz)
        to = lax.rem(z + d, nz)
        row = c4[pl.ds(to, 1), :]
        p4_send[to] = jnp.concatenate([row[:, :half], row[:, half:]], axis=0).astype(BF16)
        p4_copy(to, z, d).start()
        return 0

    lax.fori_loop(0, nz - 1, p4_start, 0)
    mine = c4[pl.ds(z, 1), :]

    def p4_wait(i, acc):
        near = i // 2 + 1
        src = lax.rem(z + nz + near * (1 - 2 * lax.rem(i, 2)), nz)
        p4_copy(z, src, 0).wait_recv()
        return acc + p4_recv[src].astype(F32)

    acc = lax.fori_loop(
        0, nz - 1, p4_wait, jnp.concatenate([mine[:, :half], mine[:, half:]], axis=0)
    )
    mixed_ref[:, :half] = (resid[:, :half] + acc[0:1]).astype(BF16)
    mixed_ref[:, half:] = (resid[:, half:] + acc[1:2]).astype(BF16)

    def p4_sent(d, _):
        p4_copy(z, z, d).wait_send()
        return 0

    lax.fori_loop(1, nz, p4_sent, 0)

    def p2_sent(d, _):
        p2_copy(m, m, d).wait_send()
        return 0

    lax.fori_loop(1, nm, p2_sent, 0)
    for k in range(3):
        for copy in w_copies(block, k):
            copy.wait_send()
    for copy in e_copies(c):
        copy.wait_send()

    def ring_sent(s, _):
        to_right(wo_v.at[e], z, s).wait_send()
        return 0

    lax.fori_loop(0, nm, ring_sent, 0)

    def ring_sent_left(s, _):
        to_left(wo_v.at[e], z, s).wait_send()
        return 0

    lax.fori_loop(0, nm - 1, ring_sent_left, 0)

    def part_sent(zz, _):
        to_part(wo_v.at[e], zz).wait_send()
        return 0

    lax.fori_loop(0, nz, part_sent, 0)


def solution(mesh):
    n = mesh.shape["ep"]
    nz = n // 2
    nm = nz // 2

    def body(
        tokens,
        cache_latent,
        cache_rope,
        lengths,
        w_query,
        w_latent,
        w_rope,
        w_absorb,
        w_value,
        w_output,
        gain_attn,
        gain_latent,
        gain_moe,
        routes,
        route_scores,
        w_gate,
        w_up,
        w_down,
    ):
        d = tokens.shape[1]
        cosine, sine = rope_tables(lengths, ROPE)
        cosine = jnp.tile(cosine, (1, 2 * HEADS))
        sine = jnp.tile(sine, (1, 2 * HEADS))
        route_weight = route_scores / jnp.sum(route_scores, axis=-1, keepdims=True)
        lanes = max(128, n)
        hits = routes[:, :, None] == jnp.arange(lanes)[None, None, :]
        table = jnp.sum(hits.astype(F32) * route_weight[:, :, None], axis=1)

        fper = w_query.shape[0]
        feats = 4 * fper
        width = w_query.shape[1] + w_latent.shape[1]
        wide = width + 128
        ff = w_gate.shape[2]
        inputs = (
            lengths,
            tokens,
            cache_latent,
            cache_rope,
            w_query,
            w_latent,
            w_rope,
            w_absorb,
            w_value,
            w_output,
            gain_attn[None, :],
            gain_latent[None, :],
            gain_moe[None, :],
            cosine,
            sine,
            table,
            w_gate,
            w_up,
            w_down,
        )
        dma = pltpu.SemaphoreType.DMA
        return pl.pallas_call(
            functools.partial(kernel, nz),
            out_shape=(
                jax.ShapeDtypeStruct((1, d), BF16),
                jax.ShapeDtypeStruct((1, LATENT), BF16),
                jax.ShapeDtypeStruct((1, ROPE), BF16),
            ),
            in_specs=[pl.BlockSpec(memory_space=pltpu.SMEM)]
            + [pl.BlockSpec(memory_space=pl.ANY)] * (len(inputs) - 1),
            out_specs=(pl.BlockSpec(memory_space=pltpu.VMEM),) * 3,
            scratch_shapes=[
                pltpu.VMEM((1, d), BF16),
                pltpu.VMEM((1, d), F32),
                pltpu.VMEM((1, LATENT), F32),
                pltpu.VMEM((1, d), F32),
                pltpu.VMEM(cosine.shape, F32),
                pltpu.VMEM(sine.shape, F32),
                pltpu.VMEM((1, lanes), F32),
                pltpu.VMEM(cache_latent.shape[1:], BF16),
                pltpu.VMEM(cache_rope.shape[1:], BF16),
                pltpu.VMEM(w_absorb.shape, BF16),
                pltpu.VMEM(w_value.shape, BF16),
                pltpu.VMEM((feats, w_query.shape[1]), BF16),
                pltpu.VMEM((feats, w_latent.shape[1]), BF16),
                pltpu.VMEM((feats, w_rope.shape[1]), BF16),
                pltpu.VMEM((n,) + w_output.shape, BF16),
                pltpu.VMEM((2, d, ff), BF16),
                pltpu.VMEM((2, d, ff), BF16),
                pltpu.VMEM((2, ff, d), BF16),
                pltpu.VMEM((nm, 1, feats), F32),
                pltpu.VMEM((nm, 1, feats), F32),
                pltpu.VMEM((nz, 1, lanes), F32),
                pltpu.VMEM((nm, 1, wide), F32),
                pltpu.VMEM((nm, 1, wide), F32),
                pltpu.VMEM((2, d // 2), BF16),
                pltpu.VMEM((nz, 2, d // 2), BF16),
                pltpu.VMEM((nz, d), F32),
                pltpu.VMEM((nz, d), F32),
                pltpu.VMEM((nz, 2, d // 2), BF16),
                pltpu.VMEM((nz, 2, d // 2), BF16),
                dma((18,)),
                dma((nm,)),
                dma((nz,)),
                dma((nz,)),
                dma((nm,)),
                dma((nz,)),
                dma((nm,)),
                dma((nz,)),
                dma((nz,)),
                dma((9,)),
                dma((12,)),
                dma((3,)),
                dma((3,)),
                dma((nm,)),
                dma((nm,)),
                dma((nm,)),
                dma((nm,)),
                dma((nz,)),
                dma((nz,)),
            ],
            compiler_params=pltpu.CompilerParams(
                collective_id=0, has_side_effects=True, vmem_limit_bytes=60 * 1024 * 1024
            ),
        )(*inputs)

    rows = P(("grp", "ep"), None)
    cached = P(("grp", "ep"), None, None)
    held = P("ep", None)
    experts = P("ep", None, None)
    return jax.shard_map(
        body,
        mesh=mesh,
        in_specs=(
            rows,
            cached,
            cached,
            P(("grp", "ep")),
            held,
            held,
            held,
            P(),
            P(),
            held,
            P(),
            P(),
            P(),
            rows,
            rows,
            experts,
            experts,
            experts,
        ),
        out_specs=(rows, rows, rows),
        check_vma=False,
    )
```

```python
import functools

import jax
import jax.numpy as jnp
import numpy as np
from jax import lax
from jax.experimental import pallas as pl
from jax.experimental.pallas import tpu as pltpu
from jax.sharding import PartitionSpec as P

HEADS = 16
NOPE = 64
ROPE = 32
VDIM = 64
LATENT = 512
EPS = 1e-06
THETA = 10000.0
MESH = pl.DeviceIdType.MESH
STEPS = (1, 3, 4)
DIGITS = (
    (0, 0, 0),
    (1, 0, 0),
    (-1, 1, 0),
    (0, 1, 0),
    (0, 0, 1),
    (1, 0, 1),
    (-1, 1, 1),
    (0, 1, 1),
    (1, 1, 1),
)
PIECES = 1
RING = (2, 5)
F32 = jnp.float32
BF16 = jnp.bfloat16


def rope_tables(position, lanes):
    place = lax.rem(lax.broadcasted_iota(jnp.int32, (1, lanes), 1), ROPE // 2)
    inverse = jnp.zeros((1, lanes), F32)
    for i in range(ROPE // 2):
        inverse = jnp.where(place == i, float(np.float32(THETA ** (-2.0 * i / ROPE))), inverse)
    angle = position.astype(F32) * inverse
    return (jnp.cos(angle), jnp.sin(angle))


def farthest_first(i, n):
    half = (i + 1) // 2
    return n // 2 + half * (1 - 2 * lax.rem(i, 2))


def rotate(x, cosine, sine):
    lanes = x.shape[-1]
    place = lax.rem(lax.broadcasted_iota(jnp.int32, x.shape, 1), ROPE)
    ahead = pltpu.roll(x, lanes - ROPE // 2, 1)
    behind = pltpu.roll(x, ROPE // 2, 1)
    return jnp.where(place < ROPE // 2, x * cosine - ahead * sine, x * cosine + behind * sine)


def dot(a, b):
    return jnp.dot(a, b, preferred_element_type=F32)


def dot_nt(a, b):
    return lax.dot_general(a, b, (((1,), (1,)), ((), ())), preferred_element_type=F32)


def kernel(
    nz,
    length_ref,
    routes_ref,
    scores_ref,
    tokens_hbm,
    cache_hbm,
    rope_hbm,
    wq_hbm,
    wl_hbm,
    wr_hbm,
    wa_hbm,
    wv_hbm,
    wo_hbm,
    gain_attn_hbm,
    gain_latent_hbm,
    gain_moe_hbm,
    wg_hbm,
    wu_hbm,
    wd_hbm,
    mixed_ref,
    new_latent_ref,
    new_rope_ref,
    tokens_v,
    gain_attn_v,
    gain_latent_v,
    gain_moe_v,
    wt_v,
    cache_v,
    rope_v,
    wa_v,
    wv_v,
    wq_v,
    wl_v,
    wr_v,
    wo_v,
    wg_v,
    wu_v,
    wd_v,
    p1_send,
    p1_recv,
    hop_send,
    hop_recv,
    wt_recv,
    p2_send,
    p2_recv,
    v_send,
    v_recv,
    o_send,
    o_recv,
    p3_send,
    p3_recv,
    x3,
    c4,
    p4_send,
    p4_recv,
    local_sem,
    send16,
    send32,
    sendw,
    send_hop,
    recv_hop,
    wt_sem,
    p2_sem,
    p3_sem,
    p4_sem,
    w_send,
    w_recv,
    e_send,
    e_recv,
    right_send,
    right_recv,
    left_send,
    left_recv,
    twin_send,
    twin_recv,
    quad_send,
    v_sem,
    o_sem,
):
    g = lax.axis_index("grp")
    q = lax.rem(g, 2)
    e = lax.axis_index("ep")
    z = e // 2
    c = lax.rem(e, 2)
    m = z // 2
    p = lax.rem(z, 2)
    nm = nz // 2
    q_width = wq_hbm.shape[1]
    lat = wl_hbm.shape[1]
    ropes = wr_hbm.shape[1]
    fper = wq_hbm.shape[0]
    feats = 4 * fper
    d_model = tokens_hbm.shape[1]
    half = d_model // 2
    cache = cache_v.shape[0]

    def dev(zz, cc):
        return (g, zz * 2 + cc)

    beside = z + 1 - 2 * p
    right = lax.rem(z + 1, nz)
    left = lax.rem(z + nz - 1, nz)

    def remote(src, dst, send, recv, to):
        return pltpu.make_async_remote_copy(
            src_ref=src, dst_ref=dst, send_sem=send, recv_sem=recv, device_id=to, device_id_type=MESH
        )

    barrier = pltpu.get_barrier_semaphore()

    near = [dev(lax.rem(z + nz + k, nz), c) for k in (1, -1, 2, -2, 4, -4)]
    near += [dev(z, 1 - c), dev(beside, 1 - c), (g + 1 - 2 * q, e)]
    for device in near:
        pl.semaphore_signal(barrier, inc=1, device_id=device, device_id_type=MESH)

    block = 2 * p + c
    rows = pl.ds(pl.multiple_of(block * fper, fper), fper)
    loads = [
        (tokens_hbm, tokens_v),
        (gain_attn_hbm, gain_attn_v),
        (wq_hbm, wq_v.at[rows]),
        (wl_hbm, wl_v.at[rows]),
        (wr_hbm, wr_v.at[rows]),
        (gain_latent_hbm, gain_latent_v),
        (gain_moe_hbm, gain_moe_v),
        (wo_hbm, wo_v.at[m]),
        (wa_hbm, wa_v),
        (cache_hbm.at[0], cache_v),
        (rope_hbm.at[0], rope_v),
        (wv_hbm, wv_v),
        (wg_hbm.at[0], wg_v.at[c]),
        (wu_hbm.at[0], wu_v.at[c]),
        (wd_hbm.at[0], wd_v.at[c]),
    ]
    local = [pltpu.make_async_copy(a, b, local_sem.at[i]) for i, (a, b) in enumerate(loads)]
    for copy in local:
        copy.start()

    local[0].wait()
    local[1].wait()
    tokens = tokens_v[...].astype(F32)
    normed = tokens * lax.rsqrt(jnp.mean(tokens * tokens, axis=-1, keepdims=True) + EPS) * gain_attn_v[...]
    normed = normed.astype(BF16).astype(F32)
    blocks = [normed[:, i * feats : (i + 1) * feats] for i in range(nm)]
    for i in range(nm):
        p1_send[i] = blocks[i]
    p1_recv[m] = p1_send[m]
    lane = lax.broadcasted_iota(jnp.int32, wt_v.shape, 1)
    first = jnp.full(wt_v.shape, scores_ref[0, 0], F32)
    second = jnp.full(wt_v.shape, scores_ref[0, 1], F32)
    both = first + second
    wt_v[...] = jnp.where(lane == routes_ref[0, 0], first / both, 0.0) + jnp.where(
        lane == routes_ref[0, 1], second / both, 0.0
    )
    wt_recv[z] = wt_v[...]
    cosine, sine = rope_tables(length_ref[0], HEADS * ROPE)
    p2_send[...] = jnp.zeros_like(p2_send)

    pl.semaphore_wait(barrier, len(near))

    w_pairs = ((wq_hbm, wq_v), (wl_hbm, wl_v), (wr_hbm, wr_v))
    w_targets = (dev(beside, c), dev(z, 1 - c))
    across = 2 * (1 - p) + c

    def w_copies(slot, k):
        at = pl.ds(pl.multiple_of(slot * fper, fper), fper)
        return [
            remote(
                src if k < 2 else dst.at[at],
                dst.at[at],
                w_send.at[3 * k + j],
                w_recv.at[3 * slot + j],
                w_targets[min(k, 1)],
            )
            for j, (src, dst) in enumerate(w_pairs)
        ]

    piece = half // PIECES

    def member(k):
        return lax.rem(m + nm + k, nm)

    def to_class(k):
        return dev(2 * member(k) + p, c)

    def lanes_of(which, k):
        return pl.ds(pl.multiple_of(which * half + k * piece, piece), piece)

    def wo_piece(mm, k):
        return wo_v.at[mm, :, lanes_of(q, k)]

    def to_twin(mm, k, which):
        part = wo_v.at[mm, :, lanes_of(which, k)]
        i = mm * PIECES + k
        return remote(part, part, twin_send.at[i], twin_recv.at[i], (g + 1 - 2 * q, e))

    def to_right(mm, s, k, src=None):
        i = s * PIECES + k
        dst = wo_piece(mm, k)
        return remote(dst if src is None else src, dst, right_send.at[i], right_recv.at[i], to_class(1))

    def to_left(mm, s, k, src=None):
        i = s * PIECES + k
        dst = wo_piece(mm, k)
        return remote(dst if src is None else src, dst, left_send.at[i], left_recv.at[i], to_class(-1))

    def ring_start():
        for k in range(PIECES):
            own = wo_hbm.at[:, lanes_of(q, k)]
            to_right(m, 0, k, own).start()
            to_left(m, 0, k, own).start()

    def ring_step(s, leftward, pass_right, pass_left):
        from_left = member(-s)
        from_right = member(s)
        for k in range(PIECES):
            to_right(from_left, s - 1, k).wait_recv()
            if pass_right:
                to_right(from_left, s, k).start()
            to_twin(from_left, k, q).start()
            if leftward:
                to_left(from_right, s - 1, k).wait_recv()
                if pass_left:
                    to_left(from_right, s, k).start()
                to_twin(from_right, k, q).start()

    def ring(first, last):
        for s in range(first, last + 1):
            ring_step(s, s < nm // 2, s < nm // 2, s < nm // 2 - 1)

    e_pairs = ((wg_hbm, wg_v), (wu_hbm, wu_v), (wd_hbm, wd_v))

    def e_copies(slot):
        return [
            remote(src.at[0], dst.at[slot], e_send.at[j], e_recv.at[j], dev(z, 1 - c))
            for j, (src, dst) in enumerate(e_pairs)
        ]

    digits = {o: DIGITS[abs(o)] if o >= 0 else tuple(-x for x in DIGITS[-o]) for o in range(1 - nm // 2, nm // 2 + 1)}
    place = {}
    for r in range(len(STEPS)):
        for sign in (1, -1):
            at = [o for o in digits if digits[o][r] == sign]
            for i, o in enumerate(at):
                place[o, r] = i

    def p1_round(r, sign):
        count = sum(1 for o in digits if digits[o][r] == sign)
        to = 2 * member(sign * STEPS[r]) + p
        i = 2 * r + (sign < 0)
        part = pl.ds(0, count)
        return remote(hop_send.at[i, part], hop_recv.at[i, part], send_hop.at[i], recv_hop.at[i], dev(to, c))

    def last_hop(o, r):
        for earlier in range(r - 1, -1, -1):
            if digits[o][earlier]:
                return earlier
        return None

    def p1_start(r):
        for o in digits:
            if digits[o][r]:
                held = last_hop(o, r)
                if held is None:
                    block_o = p1_send[member(o)]
                else:
                    block_o = hop_recv[2 * held + (digits[o][held] < 0), place[o, held]]
                hop_send[2 * r + (digits[o][r] < 0), place[o, r]] = block_o
        p1_round(r, 1).start()
        p1_round(r, -1).start()

    def p1_wait(r):
        p1_round(r, 1).wait_recv()
        p1_round(r, -1).wait_recv()

    p1_start(0)
    for k in range(2):
        for copy in w_copies(block, k):
            copy.start()
    ring_start()
    for copy in e_copies(c):
        copy.start()
    p1_wait(0)
    p1_start(1)
    for here, there in zip(w_copies(across, 0), w_copies(across, 2)):
        here.wait_recv()
        there.start()
    ring(1, RING[0])
    p1_wait(1)
    p1_start(2)
    ring(RING[0] + 1, RING[1])

    for copy in local[2:5]:
        copy.wait()
    for slot in (2 * p + 1 - c, 2 * (1 - p) + 1 - c):
        for copy in w_copies(slot, 1):
            copy.wait_recv()
    p1_wait(2)
    for o in digits:
        if o:
            held = last_hop(o, len(STEPS))
            p1_recv[member(-o)] = hop_recv[2 * held + (digits[o][held] < 0), place[o, held]]

    x1 = p1_recv[:, 0, :].astype(BF16)
    part_q = dot(x1, wq_v[...])
    part_l = dot(x1, wl_v[...])
    part_r = dot(x1, wr_v[...])
    for i in range(nm):
        p2_send[i, :, 0:q_width] = part_q[i : i + 1, :]
        p2_send[i, :, q_width : q_width + lat] = part_l[i : i + 1, :]
        p2_send[i, :, q_width + lat : q_width + lat + ropes] = part_r[i : i + 1, :]

    def p2_copy(to, slot, d):
        return remote(p2_send.at[to], p2_recv.at[slot], send16.at[d], p2_sem.at[slot], dev(2 * to + p, c))

    def p2_start(i, _):
        d = farthest_first(i, nm)
        p2_copy(lax.rem(m + d, nm), m, d).start()
        return 0

    lax.fori_loop(0, nm - 1, p2_start, 0)

    ring(RING[1] + 1, nm // 2)

    def p2_wait(i, acc):
        d = nm - 1 - i
        src = lax.rem(m + nm - d, nm)
        p2_copy(m, src, d).wait_recv()
        return acc + p2_recv[src]

    summed = lax.fori_loop(0, nm - 1, p2_wait, p2_send[m])

    for copy in local[5:7]:
        copy.wait()
    query = summed[:, :q_width].astype(BF16).astype(F32)
    latent_raw = summed[:, q_width : q_width + lat].astype(BF16).astype(F32)
    rope_raw = summed[:, q_width + lat :].astype(BF16).astype(F32)
    new_latent = (
        latent_raw
        * lax.rsqrt(jnp.mean(latent_raw * latent_raw, axis=-1, keepdims=True) + EPS)
        * gain_latent_v[...]
    ).astype(BF16)
    new_rope = rotate(rope_raw, cosine[:, : rope_raw.shape[1]], sine[:, : rope_raw.shape[1]]).astype(BF16)
    new_latent_ref[...] = new_latent
    new_rope_ref[...] = new_rope[:, :ropes]

    size = NOPE + ROPE
    q_nope = jnp.concatenate([query[:, h * size : h * size + NOPE] for h in range(HEADS)], axis=1)
    q_rope = jnp.concatenate([query[:, h * size + NOPE : (h + 1) * size] for h in range(HEADS)], axis=1)
    q_rope = rotate(q_rope, cosine, sine).astype(BF16).astype(F32)

    def by_head(row, width):
        shape = (HEADS, row.shape[1])
        own = lax.broadcasted_iota(jnp.int32, shape, 1) // width == lax.broadcasted_iota(jnp.int32, shape, 0)
        return jnp.where(own, jnp.broadcast_to(row, shape), 0.0)

    fold_shape = (HEADS * ROPE, ROPE)
    fold = (
        lax.rem(lax.broadcasted_iota(jnp.int32, fold_shape, 0), ROPE)
        == lax.broadcasted_iota(jnp.int32, fold_shape, 1)
    ).astype(F32).astype(BF16)
    q_pe = dot(by_head(q_rope, ROPE).astype(BF16), fold).astype(BF16)
    local[8].wait()
    q_abs = dot_nt(by_head(q_nope, NOPE).astype(BF16), wa_v[...]).astype(BF16)

    local[9].wait()
    local[10].wait()
    scale = (NOPE + ROPE) ** (-0.5)
    past = (dot_nt(q_abs, cache_v[...]) + dot(q_pe, rope_v[...])) * scale
    fresh = (
        jnp.sum(q_abs.astype(F32) * new_latent.astype(F32), axis=-1, keepdims=True)
        + jnp.sum(q_pe.astype(F32) * new_rope[:, :ropes].astype(F32), axis=-1, keepdims=True)
    ) * scale
    valid = lax.broadcasted_iota(jnp.int32, past.shape, 1) < length_ref[0]
    top = jnp.maximum(jnp.max(jnp.where(valid, past, -jnp.inf), axis=-1, keepdims=True), fresh)
    e_past = jnp.where(valid, jnp.exp(past - top), 0.0)
    e_new = jnp.exp(fresh - top)
    total = jnp.sum(e_past, axis=-1, keepdims=True) + e_new
    p_past = (e_past / total).astype(BF16)
    p_new = (e_new / total).astype(BF16).astype(F32)
    attended = (dot(p_past, cache_v[...]) + p_new * new_latent.astype(F32)).astype(BF16)
    local[11].wait()
    crossed = dot(attended, wv_v[...])
    own_head = (
        lax.broadcasted_iota(jnp.int32, crossed.shape, 1) // VDIM
        == lax.broadcasted_iota(jnp.int32, crossed.shape, 0)
    )
    values = jnp.sum(jnp.where(own_head, crossed, 0.0), axis=0, keepdims=True).astype(BF16)

    def beside_me(slot):
        return dev(z - p + slot // 2, lax.rem(slot, 2))

    def v_copy(slot, k):
        return remote(v_send, v_recv.at[slot], quad_send.at[k], v_sem.at[slot], beside_me(lax.rem(block + k, 4)))

    def o_copy(to, slot, k):
        return remote(o_send.at[to], o_recv.at[slot], quad_send.at[3 + k], o_sem.at[slot], beside_me(to))

    v_send[...] = values.astype(F32)
    for k in range(1, 4):
        v_copy(block, k).start()
    v_recv[block] = v_send[...]

    vals, own_rows = HEADS * VDIM, nm * wo_hbm.shape[0]
    vper = wo_hbm.shape[0]
    at = lax.broadcasted_iota(jnp.int32, (vals, own_rows), 0)
    row = lax.broadcasted_iota(jnp.int32, (vals, own_rows), 1)
    pick = (at == (4 * (row // vper) + block) * vper + lax.rem(row, vper)).astype(F32).astype(BF16)
    local[7].wait()
    for i in range(1, nm):
        for k in range(PIECES):
            to_twin(member(i), k, 1 - q).wait_recv()
    for k in range(1, 4):
        v_copy(lax.rem(block + k, 4), k).wait_recv()
    picked = dot(v_recv[:, 0, :].astype(BF16), pick).astype(BF16)
    part_o = dot(picked, wo_v[...].reshape(own_rows, d_model))
    for i in range(4):
        o_send[i] = part_o[i : i + 1, :]
    for k in range(1, 4):
        o_copy(lax.rem(block + k, 4), block, k).start()

    def wt_copy(to, slot, d):
        return remote(wt_v, wt_recv.at[slot], sendw.at[d], wt_sem.at[slot], dev(to, c))

    def wt_start(i, _):
        d = farthest_first(i, nz)
        wt_copy(lax.rem(z + d, nz), z, d).start()
        return 0

    lax.fori_loop(0, nz - 1, wt_start, 0)

    attn_out = o_send[block]
    for k in range(1, 4):
        slot = lax.rem(block + k, 4)
        o_copy(block, slot, k).wait_recv()
        attn_out = attn_out + o_recv[slot]
    resid = (tokens + attn_out).astype(BF16).astype(F32)
    moe_in = resid * lax.rsqrt(jnp.mean(resid * resid, axis=-1, keepdims=True) + EPS) * gain_moe_v[...]
    moe_in = moe_in.astype(BF16).astype(F32)
    p3_send[...] = jnp.concatenate([moe_in[:, :half], moe_in[:, half:]], axis=0).astype(BF16)

    def p3_copy(to, slot, d):
        return remote(p3_send, p3_recv.at[slot], send32.at[d], p3_sem.at[slot], dev(to, c))

    def p3_start(i, _):
        d = farthest_first(i, nz)
        p3_copy(lax.rem(z + d, nz), z, d).start()
        return 0

    lax.fori_loop(0, nz - 1, p3_start, 0)
    x3[pl.ds(z, 1), :] = moe_in

    for copy in local[12:15]:
        copy.wait()
    for copy in e_copies(1 - c):
        copy.wait_recv()

    def wt_wait(i, _):
        d = i + 1
        wt_copy(z, lax.rem(z + nz - d, nz), d).wait()
        return 0

    lax.fori_loop(0, nz - 1, wt_wait, 0)

    def p3_wait(i, _):
        near = i // 2 + 1
        src = lax.rem(z + nz + near * (1 - 2 * lax.rem(i, 2)), nz)
        p3_copy(z, src, 0).wait_recv()
        row = p3_recv[src].astype(F32)
        x3[pl.ds(src, 1), 0:half] = row[0:1]
        x3[pl.ds(src, 1), half:d_model] = row[1:2]
        return 0

    lax.fori_loop(0, nz - 1, p3_wait, 0)

    def p3_sent(d, _):
        p3_copy(z, z, d).wait_send()
        return 0

    lax.fori_loop(1, nz, p3_sent, 0)

    rows3 = x3[...].astype(BF16)
    shares = wt_recv[:, 0, :]
    expert = lax.broadcasted_iota(jnp.int32, shares.shape, 1)
    outs = []
    for s in range(2):
        share = jnp.sum(jnp.where(expert == 2 * z + s, shares, 0.0), axis=1, keepdims=True)
        gate = dot(rows3, wg_v[s])
        upper = dot(rows3, wu_v[s])
        hidden = (jax.nn.silu(gate) * upper).astype(BF16)
        result = dot(hidden, wd_v[s]).astype(BF16).astype(F32)
        outs.append(share * result)
    c4[...] = outs[0] + outs[1]

    def p4_copy(to, slot, d):
        return remote(p4_send.at[to], p4_recv.at[slot], send32.at[d], p4_sem.at[slot], dev(to, c))

    def p4_start(i, _):
        d = farthest_first(i, nz)
        to = lax.rem(z + d, nz)
        row = c4[pl.ds(to, 1), :]
        p4_send[to] = jnp.concatenate([row[:, :half], row[:, half:]], axis=0).astype(BF16)
        p4_copy(to, z, d).start()
        return 0

    lax.fori_loop(0, nz - 1, p4_start, 0)
    mine = c4[pl.ds(z, 1), :]

    def p4_wait(i, acc):
        near = i // 2 + 1
        src = lax.rem(z + nz + near * (1 - 2 * lax.rem(i, 2)), nz)
        p4_copy(z, src, 0).wait_recv()
        return acc + p4_recv[src].astype(F32)

    acc = lax.fori_loop(
        0, nz - 1, p4_wait, jnp.concatenate([mine[:, :half], mine[:, half:]], axis=0)
    )
    mixed_ref[:, :half] = (resid[:, :half] + acc[0:1]).astype(BF16)
    mixed_ref[:, half:] = (resid[:, half:] + acc[1:2]).astype(BF16)

    def p4_sent(d, _):
        p4_copy(z, z, d).wait_send()
        return 0

    lax.fori_loop(1, nz, p4_sent, 0)

    def p2_sent(d, _):
        p2_copy(m, m, d).wait_send()
        return 0

    lax.fori_loop(1, nm, p2_sent, 0)
    for k in range(2):
        for copy in w_copies(block, k):
            copy.wait_send()
    for copy in w_copies(across, 2):
        copy.wait_send()
    for copy in e_copies(c):
        copy.wait_send()

    for i in range(nm // 2):
        for k in range(PIECES):
            to_right(m, i, k).wait_send()
            if i < nm // 2 - 1:
                to_left(m, i, k).wait_send()
    for i in range(1, nm):
        for k in range(PIECES):
            to_twin(member(i), k, q).wait_send()
    for k in range(1, 4):
        v_copy(block, k).wait_send()
        o_copy(block, block, k).wait_send()
    for r in range(len(STEPS)):
        p1_round(r, 1).wait_send()
        p1_round(r, -1).wait_send()


def hand_over(a, b, c, x, y, w):
    x[...] = a[...]
    y[...] = b[...]
    w[...] = c[...]


def solution(mesh):
    n = mesh.shape["ep"]
    nz = n // 2
    nm = nz // 2

    def body(
        tokens,
        cache_latent,
        cache_rope,
        lengths,
        w_query,
        w_latent,
        w_rope,
        w_absorb,
        w_value,
        w_output,
        gain_attn,
        gain_latent,
        gain_moe,
        routes,
        route_scores,
        w_gate,
        w_up,
        w_down,
    ):
        d = tokens.shape[1]
        lanes = max(128, n)
        fper = w_query.shape[0]
        feats = 4 * fper
        width = w_query.shape[1] + w_latent.shape[1]
        wide = width + 128
        ff = w_gate.shape[2]
        inputs = (
            lengths,
            routes,
            route_scores,
            tokens,
            cache_latent,
            cache_rope,
            w_query,
            w_latent,
            w_rope,
            w_absorb,
            w_value,
            w_output,
            gain_attn[None, :],
            gain_latent[None, :],
            gain_moe[None, :],
            w_gate,
            w_up,
            w_down,
        )
        dma = pltpu.SemaphoreType.DMA
        outs = pl.pallas_call(
            functools.partial(kernel, nz),
            out_shape=(
                jax.ShapeDtypeStruct((1, d), BF16),
                jax.ShapeDtypeStruct((1, LATENT), BF16),
                jax.ShapeDtypeStruct((1, ROPE), BF16),
            ),
            in_specs=[pl.BlockSpec(memory_space=pltpu.SMEM)] * 3
            + [pl.BlockSpec(memory_space=pl.ANY)] * (len(inputs) - 3),
            out_specs=(pl.BlockSpec(memory_space=pltpu.VMEM),) * 3,
            scratch_shapes=[
                pltpu.VMEM((1, d), BF16),
                pltpu.VMEM((1, d), F32),
                pltpu.VMEM((1, LATENT), F32),
                pltpu.VMEM((1, d), F32),
                pltpu.VMEM((1, lanes), F32),
                pltpu.VMEM(cache_latent.shape[1:], BF16),
                pltpu.VMEM(cache_rope.shape[1:], BF16),
                pltpu.VMEM(w_absorb.shape, BF16),
                pltpu.VMEM(w_value.shape, BF16),
                pltpu.VMEM((feats, w_query.shape[1]), BF16),
                pltpu.VMEM((feats, w_latent.shape[1]), BF16),
                pltpu.VMEM((feats, w_rope.shape[1]), BF16),
                pltpu.VMEM((nm,) + w_output.shape, BF16),
                pltpu.VMEM((2, d, ff), BF16),
                pltpu.VMEM((2, d, ff), BF16),
                pltpu.VMEM((2, ff, d), BF16),
                pltpu.VMEM((nm, 1, feats), F32),
                pltpu.VMEM((nm, 1, feats), F32),
                pltpu.VMEM((6, 5, 1, feats), F32),
                pltpu.VMEM((6, 5, 1, feats), F32),
                pltpu.VMEM((nz, 1, lanes), F32),
                pltpu.VMEM((nm, 1, wide), F32),
                pltpu.VMEM((nm, 1, wide), F32),
                pltpu.VMEM((1, HEADS * VDIM), F32),
                pltpu.VMEM((4, 1, HEADS * VDIM), F32),
                pltpu.VMEM((4, 1, d), F32),
                pltpu.VMEM((4, 1, d), F32),
                pltpu.VMEM((2, d // 2), BF16),
                pltpu.VMEM((nz, 2, d // 2), BF16),
                pltpu.VMEM((nz, d), F32),
                pltpu.VMEM((nz, d), F32),
                pltpu.VMEM((nz, 2, d // 2), BF16),
                pltpu.VMEM((nz, 2, d // 2), BF16),
                dma((15,)),
                dma((nm,)),
                dma((nz,)),
                dma((nz,)),
                dma((6,)),
                dma((6,)),
                dma((nz,)),
                dma((nm,)),
                dma((nz,)),
                dma((nz,)),
                dma((9,)),
                dma((12,)),
                dma((3,)),
                dma((3,)),
                dma((nm // 2 * PIECES,)),
                dma((nm // 2 * PIECES,)),
                dma((nm // 2 * PIECES,)),
                dma((nm // 2 * PIECES,)),
                dma((nm * PIECES,)),
                dma((nm * PIECES,)),
                dma((7,)),
                dma((4,)),
                dma((4,)),
            ],
            compiler_params=pltpu.CompilerParams(
                collective_id=0, has_side_effects=True, vmem_limit_bytes=60 * 1024 * 1024
            ),
        )(*inputs)
        return pl.pallas_call(
            hand_over,
            out_shape=tuple(jax.ShapeDtypeStruct(o.shape, o.dtype) for o in outs),
            in_specs=[pl.BlockSpec(memory_space=pltpu.VMEM)] * 3,
            out_specs=(pl.BlockSpec(memory_space=pltpu.VMEM),) * 3,
        )(*outs)

    rows = P(("grp", "ep"), None)
    cached = P(("grp", "ep"), None, None)
    held = P("ep", None)
    experts = P("ep", None, None)
    return jax.shard_map(
        body,
        mesh=mesh,
        in_specs=(
            rows,
            cached,
            cached,
            P(("grp", "ep")),
            held,
            held,
            held,
            P(),
            P(),
            held,
            P(),
            P(),
            P(),
            rows,
            rows,
            experts,
            experts,
            experts,
        ),
        out_specs=(rows, rows, rows),
        check_vma=False,
    )
```

```python
import functools

import jax
import jax.numpy as jnp
import numpy as np
from jax import lax
from jax.experimental import pallas as pl
from jax.experimental.pallas import tpu as pltpu
from jax.sharding import PartitionSpec as P

HEADS = 16
NOPE = 64
ROPE = 32
VDIM = 64
LATENT = 512
EPS = 1e-06
THETA = 10000.0
MESH = pl.DeviceIdType.MESH
STEPS = (1, 3, 4)
DIGITS = (
    (0, 0, 0),
    (1, 0, 0),
    (-1, 1, 0),
    (0, 1, 0),
    (0, 0, 1),
    (1, 0, 1),
    (-1, 1, 1),
    (0, 1, 1),
    (1, 1, 1),
)
PIECES = 1
RING = (2, 4)
F32 = jnp.float32
BF16 = jnp.bfloat16


def rope_tables(position, lanes):
    place = lax.rem(lax.broadcasted_iota(jnp.int32, (1, lanes), 1), ROPE // 2)
    inverse = jnp.zeros((1, lanes), F32)
    for i in range(ROPE // 2):
        inverse = jnp.where(place == i, float(np.float32(THETA ** (-2.0 * i / ROPE))), inverse)
    angle = position.astype(F32) * inverse
    return (jnp.cos(angle), jnp.sin(angle))


def farthest_first(i, n):
    half = (i + 1) // 2
    return n // 2 + half * (1 - 2 * lax.rem(i, 2))


def rotate(x, cosine, sine):
    lanes = x.shape[-1]
    place = lax.rem(lax.broadcasted_iota(jnp.int32, x.shape, 1), ROPE)
    ahead = pltpu.roll(x, lanes - ROPE // 2, 1)
    behind = pltpu.roll(x, ROPE // 2, 1)
    return jnp.where(place < ROPE // 2, x * cosine - ahead * sine, x * cosine + behind * sine)


def dot(a, b):
    return jnp.dot(a, b, preferred_element_type=F32)


def dot_nt(a, b):
    return lax.dot_general(a, b, (((1,), (1,)), ((), ())), preferred_element_type=F32)


def kernel(
    nz,
    length_ref,
    routes_ref,
    scores_ref,
    tokens_hbm,
    cache_hbm,
    rope_hbm,
    wq_hbm,
    wl_hbm,
    wr_hbm,
    wa_hbm,
    wv_hbm,
    wo_hbm,
    gain_attn_hbm,
    gain_latent_hbm,
    gain_moe_hbm,
    wg_hbm,
    wu_hbm,
    wd_hbm,
    mixed_ref,
    new_latent_ref,
    new_rope_ref,
    tokens_v,
    gain_attn_v,
    gain_latent_v,
    gain_moe_v,
    wt_v,
    cache_v,
    rope_v,
    wa_v,
    wv_v,
    wq_v,
    wl_v,
    wr_v,
    wo_v,
    wg_v,
    wu_v,
    wd_v,
    p1_send,
    p1_recv,
    hop_send,
    hop_recv,
    wt_recv,
    p2_send,
    p2_recv,
    p2r_send,
    p2r_recv,
    v_send,
    v_recv,
    o_send,
    o_recv,
    p3_send,
    p3_recv,
    x3,
    c4,
    p4_send,
    p4_recv,
    local_sem,
    send16,
    send16r,
    send32,
    sendw,
    send_hop,
    recv_hop,
    wt_sem,
    p2_sem,
    p2r_sem,
    p3_sem,
    p4_sem,
    w_send,
    w_recv,
    e_send,
    e_recv,
    right_send,
    right_recv,
    left_send,
    left_recv,
    twin_send,
    twin_recv,
    quad_send,
    v_sem,
    o_sem,
):
    g = lax.axis_index("grp")
    q = lax.rem(g, 2)
    e = lax.axis_index("ep")
    z = e // 2
    c = lax.rem(e, 2)
    m = z // 2
    p = lax.rem(z, 2)
    nm = nz // 2
    ropes = wr_hbm.shape[1]
    fper = wq_hbm.shape[0]
    feats = 4 * fper
    d_model = tokens_hbm.shape[1]
    half = d_model // 2
    cache = cache_v.shape[0]

    def dev(zz, cc):
        return (g, zz * 2 + cc)

    beside = z + 1 - 2 * p
    right = lax.rem(z + 1, nz)
    left = lax.rem(z + nz - 1, nz)

    def remote(src, dst, send, recv, to):
        return pltpu.make_async_remote_copy(
            src_ref=src, dst_ref=dst, send_sem=send, recv_sem=recv, device_id=to, device_id_type=MESH
        )

    barrier = pltpu.get_barrier_semaphore()

    near = [dev(lax.rem(z + nz + k, nz), c) for k in (1, -1, 2, -2, 4, -4)]
    near += [dev(z, 1 - c), dev(beside, 1 - c), (g + 1 - 2 * q, e)]
    for device in near:
        pl.semaphore_signal(barrier, inc=1, device_id=device, device_id_type=MESH)

    block = 2 * p + c
    rows = pl.ds(pl.multiple_of(block * fper, fper), fper)
    loads = [
        (tokens_hbm, tokens_v),
        (gain_attn_hbm, gain_attn_v),
        (wq_hbm, wq_v.at[rows]),
        (wl_hbm, wl_v.at[rows]),
        (wr_hbm, wr_v.at[rows]),
        (gain_latent_hbm, gain_latent_v),
        (gain_moe_hbm, gain_moe_v),
        (wo_hbm, wo_v.at[m]),
        (wa_hbm, wa_v),
        (cache_hbm.at[0], cache_v),
        (rope_hbm.at[0], rope_v),
        (wv_hbm, wv_v),
        (wg_hbm.at[0], wg_v.at[c]),
        (wu_hbm.at[0], wu_v.at[c]),
        (wd_hbm.at[0], wd_v.at[c]),
    ]
    local = [pltpu.make_async_copy(a, b, local_sem.at[i]) for i, (a, b) in enumerate(loads)]
    for copy in local:
        copy.start()

    local[0].wait()
    local[1].wait()
    tokens = tokens_v[...].astype(F32)
    normed = tokens * lax.rsqrt(jnp.mean(tokens * tokens, axis=-1, keepdims=True) + EPS) * gain_attn_v[...]
    normed = normed.astype(BF16).astype(F32)
    blocks = [normed[:, i * feats : (i + 1) * feats] for i in range(nm)]
    for i in range(nm):
        p1_send[i] = blocks[i]
    p1_recv[m] = p1_send[m]
    lane = lax.broadcasted_iota(jnp.int32, wt_v.shape, 1)
    first = jnp.full(wt_v.shape, scores_ref[0, 0], F32)
    second = jnp.full(wt_v.shape, scores_ref[0, 1], F32)
    both = first + second
    wt_v[...] = jnp.where(lane == routes_ref[0, 0], first / both, 0.0) + jnp.where(
        lane == routes_ref[0, 1], second / both, 0.0
    )
    wt_recv[z] = wt_v[...]
    cosine, sine = rope_tables(length_ref[0], HEADS * ROPE)
    p2r_send[...] = jnp.zeros_like(p2r_send)

    pl.semaphore_wait(barrier, len(near))

    w_pairs = ((wq_hbm, wq_v), (wl_hbm, wl_v), (wr_hbm, wr_v))
    w_targets = (dev(beside, c), dev(z, 1 - c))
    across = 2 * (1 - p) + c

    def w_copies(slot, k):
        at = pl.ds(pl.multiple_of(slot * fper, fper), fper)
        return [
            remote(
                src if k < 2 else dst.at[at],
                dst.at[at],
                w_send.at[3 * k + j],
                w_recv.at[3 * slot + j],
                w_targets[min(k, 1)],
            )
            for j, (src, dst) in enumerate(w_pairs)
        ]

    piece = half // PIECES

    def member(k):
        return lax.rem(m + nm + k, nm)

    def to_class(k):
        return dev(2 * member(k) + p, c)

    def lanes_of(which, k):
        return pl.ds(pl.multiple_of(which * half + k * piece, piece), piece)

    def wo_piece(mm, k):
        return wo_v.at[mm, :, lanes_of(q, k)]

    def to_twin(mm, k, which):
        part = wo_v.at[mm, :, lanes_of(which, k)]
        i = mm * PIECES + k
        return remote(part, part, twin_send.at[i], twin_recv.at[i], (g + 1 - 2 * q, e))

    def to_right(mm, s, k, src=None):
        i = s * PIECES + k
        dst = wo_piece(mm, k)
        return remote(dst if src is None else src, dst, right_send.at[i], right_recv.at[i], to_class(1))

    def to_left(mm, s, k, src=None):
        i = s * PIECES + k
        dst = wo_piece(mm, k)
        return remote(dst if src is None else src, dst, left_send.at[i], left_recv.at[i], to_class(-1))

    def ring_start():
        for k in range(PIECES):
            own = wo_hbm.at[:, lanes_of(q, k)]
            to_right(m, 0, k, own).start()
            to_left(m, 0, k, own).start()

    def ring_step(s, leftward, pass_right, pass_left):
        from_left = member(-s)
        from_right = member(s)
        for k in range(PIECES):
            to_right(from_left, s - 1, k).wait_recv()
            if pass_right:
                to_right(from_left, s, k).start()
            to_twin(from_left, k, q).start()
            if leftward:
                to_left(from_right, s - 1, k).wait_recv()
                if pass_left:
                    to_left(from_right, s, k).start()
                to_twin(from_right, k, q).start()

    def ring(first, last):
        for s in range(first, last + 1):
            ring_step(s, s < nm // 2, s < nm // 2, s < nm // 2 - 1)

    e_pairs = ((wg_hbm, wg_v), (wu_hbm, wu_v), (wd_hbm, wd_v))

    def e_copies(slot):
        return [
            remote(src.at[0], dst.at[slot], e_send.at[j], e_recv.at[j], dev(z, 1 - c))
            for j, (src, dst) in enumerate(e_pairs)
        ]

    digits = {o: DIGITS[abs(o)] if o >= 0 else tuple(-x for x in DIGITS[-o]) for o in range(1 - nm // 2, nm // 2 + 1)}
    place = {}
    for r in range(len(STEPS)):
        for sign in (1, -1):
            at = [o for o in digits if digits[o][r] == sign]
            for i, o in enumerate(at):
                place[o, r] = i

    def p1_round(r, sign):
        count = sum(1 for o in digits if digits[o][r] == sign)
        to = 2 * member(sign * STEPS[r]) + p
        i = 2 * r + (sign < 0)
        part = pl.ds(0, count)
        return remote(hop_send.at[i, part], hop_recv.at[i, part], send_hop.at[i], recv_hop.at[i], dev(to, c))

    def last_hop(o, r):
        for earlier in range(r - 1, -1, -1):
            if digits[o][earlier]:
                return earlier
        return None

    def p1_start(r):
        for o in digits:
            if digits[o][r]:
                held = last_hop(o, r)
                if held is None:
                    block_o = p1_send[member(o)]
                else:
                    block_o = hop_recv[2 * held + (digits[o][held] < 0), place[o, held]]
                hop_send[2 * r + (digits[o][r] < 0), place[o, r]] = block_o
        p1_round(r, 1).start()
        p1_round(r, -1).start()

    def p1_wait(r):
        p1_round(r, 1).wait_recv()
        p1_round(r, -1).wait_recv()

    p1_start(0)
    for k in range(2):
        for copy in w_copies(block, k):
            copy.start()
    ring_start()
    for copy in e_copies(c):
        copy.start()
    p1_wait(0)
    p1_start(1)
    for here, there in zip(w_copies(across, 0), w_copies(across, 2)):
        here.wait_recv()
        there.start()
    ring(1, RING[0])
    p1_wait(1)
    p1_start(2)
    ring(RING[0] + 1, RING[1])

    for copy in local[2:5]:
        copy.wait()
    for slot in (2 * p + 1 - c, 2 * (1 - p) + 1 - c):
        for copy in w_copies(slot, 1):
            copy.wait_recv()
    p1_wait(2)
    for o in digits:
        if o:
            held = last_hop(o, len(STEPS))
            p1_recv[member(-o)] = hop_recv[2 * held + (digits[o][held] < 0), place[o, held]]

    x1 = p1_recv[:, 0, :].astype(BF16)
    part_q = dot(x1, wq_v[...])
    part_l = dot(x1, wl_v[...])
    part_r = dot(x1, wr_v[...])
    size = NOPE + ROPE
    nope, turned = HEADS * NOPE, HEADS * ROPE
    part_n = jnp.concatenate([part_q[:, h * size : h * size + NOPE] for h in range(HEADS)], axis=1)
    part_p = jnp.concatenate([part_q[:, h * size + NOPE : (h + 1) * size] for h in range(HEADS)], axis=1)
    plain = jnp.concatenate([part_n, part_l], axis=1)
    fold2 = plain.shape[1] // 2
    for i in range(nm):
        row = plain[i : i + 1, :]
        p2_send[i] = jnp.concatenate([row[:, :fold2], row[:, fold2:]], axis=0).astype(BF16)
        p2r_send[i, :, 0:turned] = part_p[i : i + 1, :]
        p2r_send[i, :, turned : turned + ropes] = part_r[i : i + 1, :]

    def p2_copy(to, slot, d):
        return remote(p2_send.at[to], p2_recv.at[slot], send16.at[d], p2_sem.at[slot], dev(2 * to + p, c))

    def p2r_copy(to, slot, d):
        return remote(p2r_send.at[to], p2r_recv.at[slot], send16r.at[d], p2r_sem.at[slot], dev(2 * to + p, c))

    def p2_start(i, _):
        d = farthest_first(i, nm)
        to = lax.rem(m + d, nm)
        p2r_copy(to, m, d).start()
        p2_copy(to, m, d).start()
        return 0

    lax.fori_loop(0, nm - 1, p2_start, 0)

    ring(RING[1] + 1, nm // 2 - 1)

    def p2_wait(i, acc):
        d = nm - 1 - i
        src = lax.rem(m + nm - d, nm)
        p2r_copy(m, src, d).wait_recv()
        p2_copy(m, src, d).wait_recv()
        return (acc[0] + p2_recv[src].astype(F32), acc[1] + p2r_recv[src])

    folded, turns = lax.fori_loop(0, nm - 1, p2_wait, (p2_send[m].astype(F32), p2r_send[m]))
    summed = jnp.concatenate([folded[0:1], folded[1:2]], axis=1)

    for copy in local[5:7]:
        copy.wait()
    q_nope = summed[:, :nope].astype(BF16).astype(F32)
    q_rope = turns[:, :turned].astype(BF16).astype(F32)
    latent_raw = summed[:, nope:].astype(BF16).astype(F32)
    rope_raw = turns[:, turned:].astype(BF16).astype(F32)
    new_latent = (
        latent_raw
        * lax.rsqrt(jnp.mean(latent_raw * latent_raw, axis=-1, keepdims=True) + EPS)
        * gain_latent_v[...]
    ).astype(BF16)
    new_rope = rotate(rope_raw, cosine[:, : rope_raw.shape[1]], sine[:, : rope_raw.shape[1]]).astype(BF16)
    new_latent_ref[...] = new_latent
    new_rope_ref[...] = new_rope[:, :ropes]

    q_rope = rotate(q_rope, cosine, sine).astype(BF16).astype(F32)

    def by_head(row, width):
        shape = (HEADS, row.shape[1])
        own = lax.broadcasted_iota(jnp.int32, shape, 1) // width == lax.broadcasted_iota(jnp.int32, shape, 0)
        return jnp.where(own, jnp.broadcast_to(row, shape), 0.0)

    fold_shape = (HEADS * ROPE, ROPE)
    fold = (
        lax.rem(lax.broadcasted_iota(jnp.int32, fold_shape, 0), ROPE)
        == lax.broadcasted_iota(jnp.int32, fold_shape, 1)
    ).astype(F32).astype(BF16)
    q_pe = dot(by_head(q_rope, ROPE).astype(BF16), fold).astype(BF16)
    local[8].wait()
    q_abs = dot_nt(by_head(q_nope, NOPE).astype(BF16), wa_v[...]).astype(BF16)

    local[9].wait()
    local[10].wait()
    scale = (NOPE + ROPE) ** (-0.5)
    past = (dot_nt(q_abs, cache_v[...]) + dot(q_pe, rope_v[...])) * scale
    fresh = (
        jnp.sum(q_abs.astype(F32) * new_latent.astype(F32), axis=-1, keepdims=True)
        + jnp.sum(q_pe.astype(F32) * new_rope[:, :ropes].astype(F32), axis=-1, keepdims=True)
    ) * scale
    valid = lax.broadcasted_iota(jnp.int32, past.shape, 1) < length_ref[0]
    top = jnp.maximum(jnp.max(jnp.where(valid, past, -jnp.inf), axis=-1, keepdims=True), fresh)
    e_past = jnp.where(valid, jnp.exp(past - top), 0.0)
    e_new = jnp.exp(fresh - top)
    total = jnp.sum(e_past, axis=-1, keepdims=True) + e_new
    p_past = (e_past / total).astype(BF16)
    p_new = (e_new / total).astype(BF16).astype(F32)
    attended = (dot(p_past, cache_v[...]) + p_new * new_latent.astype(F32)).astype(BF16)
    local[11].wait()
    crossed = dot(attended, wv_v[...])
    own_head = (
        lax.broadcasted_iota(jnp.int32, crossed.shape, 1) // VDIM
        == lax.broadcasted_iota(jnp.int32, crossed.shape, 0)
    )
    values = jnp.sum(jnp.where(own_head, crossed, 0.0), axis=0, keepdims=True).astype(BF16)

    def beside_me(slot):
        return dev(z - p + slot // 2, lax.rem(slot, 2))

    def v_copy(slot, k):
        return remote(v_send, v_recv.at[slot], quad_send.at[k], v_sem.at[slot], beside_me(lax.rem(block + k, 4)))

    def o_copy(to, slot, k):
        return remote(o_send.at[to], o_recv.at[slot], quad_send.at[3 + k], o_sem.at[slot], beside_me(to))

    v_send[...] = values.astype(F32)
    for k in range(1, 4):
        v_copy(block, k).start()
    v_recv[block] = v_send[...]
    ring(nm // 2, nm // 2)

    vals, own_rows = HEADS * VDIM, nm * wo_hbm.shape[0]
    vper = wo_hbm.shape[0]
    at = lax.broadcasted_iota(jnp.int32, (vals, own_rows), 0)
    row = lax.broadcasted_iota(jnp.int32, (vals, own_rows), 1)
    pick = (at == (4 * (row // vper) + block) * vper + lax.rem(row, vper)).astype(F32).astype(BF16)
    local[7].wait()
    for i in range(1, nm):
        for k in range(PIECES):
            to_twin(member(i), k, 1 - q).wait_recv()
    for k in range(1, 4):
        v_copy(lax.rem(block + k, 4), k).wait_recv()
    picked = dot(v_recv[:, 0, :].astype(BF16), pick).astype(BF16)
    part_o = dot(picked, wo_v[...].reshape(own_rows, d_model))
    for i in range(4):
        o_send[i] = part_o[i : i + 1, :]
    for k in range(1, 4):
        o_copy(lax.rem(block + k, 4), block, k).start()

    def wt_copy(to, slot, d):
        return remote(wt_v, wt_recv.at[slot], sendw.at[d], wt_sem.at[slot], dev(to, c))

    def wt_start(i, _):
        d = farthest_first(i, nz)
        wt_copy(lax.rem(z + d, nz), z, d).start()
        return 0

    lax.fori_loop(0, nz - 1, wt_start, 0)

    attn_out = o_send[block]
    for k in range(1, 4):
        slot = lax.rem(block + k, 4)
        o_copy(block, slot, k).wait_recv()
        attn_out = attn_out + o_recv[slot]
    resid = (tokens + attn_out).astype(BF16).astype(F32)
    moe_in = resid * lax.rsqrt(jnp.mean(resid * resid, axis=-1, keepdims=True) + EPS) * gain_moe_v[...]
    moe_in = moe_in.astype(BF16).astype(F32)
    p3_send[...] = jnp.concatenate([moe_in[:, :half], moe_in[:, half:]], axis=0).astype(BF16)

    def p3_copy(to, slot, d):
        return remote(p3_send, p3_recv.at[slot], send32.at[d], p3_sem.at[slot], dev(to, c))

    def p3_start(i, _):
        d = farthest_first(i, nz)
        p3_copy(lax.rem(z + d, nz), z, d).start()
        return 0

    lax.fori_loop(0, nz - 1, p3_start, 0)
    x3[pl.ds(z, 1), :] = moe_in

    for copy in local[12:15]:
        copy.wait()
    for copy in e_copies(1 - c):
        copy.wait_recv()

    def wt_wait(i, _):
        d = i + 1
        wt_copy(z, lax.rem(z + nz - d, nz), d).wait()
        return 0

    lax.fori_loop(0, nz - 1, wt_wait, 0)

    def p3_wait(i, _):
        near = i // 2 + 1
        src = lax.rem(z + nz + near * (1 - 2 * lax.rem(i, 2)), nz)
        p3_copy(z, src, 0).wait_recv()
        row = p3_recv[src].astype(F32)
        x3[pl.ds(src, 1), 0:half] = row[0:1]
        x3[pl.ds(src, 1), half:d_model] = row[1:2]
        return 0

    lax.fori_loop(0, nz - 1, p3_wait, 0)

    def p3_sent(d, _):
        p3_copy(z, z, d).wait_send()
        return 0

    lax.fori_loop(1, nz, p3_sent, 0)

    rows3 = x3[...].astype(BF16)
    shares = wt_recv[:, 0, :]
    expert = lax.broadcasted_iota(jnp.int32, shares.shape, 1)
    outs = []
    for s in range(2):
        share = jnp.sum(jnp.where(expert == 2 * z + s, shares, 0.0), axis=1, keepdims=True)
        gate = dot(rows3, wg_v[s])
        upper = dot(rows3, wu_v[s])
        hidden = (jax.nn.silu(gate) * upper).astype(BF16)
        result = dot(hidden, wd_v[s]).astype(BF16).astype(F32)
        outs.append(share * result)
    c4[...] = outs[0] + outs[1]

    def p4_copy(to, slot, d):
        return remote(p4_send.at[to], p4_recv.at[slot], send32.at[d], p4_sem.at[slot], dev(to, c))

    def p4_start(i, _):
        d = farthest_first(i, nz)
        to = lax.rem(z + d, nz)
        row = c4[pl.ds(to, 1), :]
        p4_send[to] = jnp.concatenate([row[:, :half], row[:, half:]], axis=0).astype(BF16)
        p4_copy(to, z, d).start()
        return 0

    lax.fori_loop(0, nz - 1, p4_start, 0)
    mine = c4[pl.ds(z, 1), :]

    def p4_wait(i, acc):
        near = i // 2 + 1
        src = lax.rem(z + nz + near * (1 - 2 * lax.rem(i, 2)), nz)
        p4_copy(z, src, 0).wait_recv()
        return acc + p4_recv[src].astype(F32)

    acc = lax.fori_loop(
        0, nz - 1, p4_wait, jnp.concatenate([mine[:, :half], mine[:, half:]], axis=0)
    )
    mixed_ref[:, :half] = (resid[:, :half] + acc[0:1]).astype(BF16)
    mixed_ref[:, half:] = (resid[:, half:] + acc[1:2]).astype(BF16)

    def p4_sent(d, _):
        p4_copy(z, z, d).wait_send()
        return 0

    lax.fori_loop(1, nz, p4_sent, 0)

    def p2_sent(d, _):
        p2_copy(m, m, d).wait_send()
        p2r_copy(m, m, d).wait_send()
        return 0

    lax.fori_loop(1, nm, p2_sent, 0)
    for k in range(2):
        for copy in w_copies(block, k):
            copy.wait_send()
    for copy in w_copies(across, 2):
        copy.wait_send()
    for copy in e_copies(c):
        copy.wait_send()

    for i in range(nm // 2):
        for k in range(PIECES):
            to_right(m, i, k).wait_send()
            if i < nm // 2 - 1:
                to_left(m, i, k).wait_send()
    for i in range(1, nm):
        for k in range(PIECES):
            to_twin(member(i), k, q).wait_send()
    for k in range(1, 4):
        v_copy(block, k).wait_send()
        o_copy(block, block, k).wait_send()
    for r in range(len(STEPS)):
        p1_round(r, 1).wait_send()
        p1_round(r, -1).wait_send()


def hand_over(a, b, c, x, y, w):
    x[...] = a[...]
    y[...] = b[...]
    w[...] = c[...]


def solution(mesh):
    n = mesh.shape["ep"]
    nz = n // 2
    nm = nz // 2

    def body(
        tokens,
        cache_latent,
        cache_rope,
        lengths,
        w_query,
        w_latent,
        w_rope,
        w_absorb,
        w_value,
        w_output,
        gain_attn,
        gain_latent,
        gain_moe,
        routes,
        route_scores,
        w_gate,
        w_up,
        w_down,
    ):
        d = tokens.shape[1]
        lanes = max(128, n)
        fper = w_query.shape[0]
        feats = 4 * fper
        plain = HEADS * NOPE + w_latent.shape[1]
        turned = HEADS * ROPE + 128
        ff = w_gate.shape[2]
        inputs = (
            lengths,
            routes,
            route_scores,
            tokens,
            cache_latent,
            cache_rope,
            w_query,
            w_latent,
            w_rope,
            w_absorb,
            w_value,
            w_output,
            gain_attn[None, :],
            gain_latent[None, :],
            gain_moe[None, :],
            w_gate,
            w_up,
            w_down,
        )
        dma = pltpu.SemaphoreType.DMA
        outs = pl.pallas_call(
            functools.partial(kernel, nz),
            out_shape=(
                jax.ShapeDtypeStruct((1, d), BF16),
                jax.ShapeDtypeStruct((1, LATENT), BF16),
                jax.ShapeDtypeStruct((1, ROPE), BF16),
            ),
            in_specs=[pl.BlockSpec(memory_space=pltpu.SMEM)] * 3
            + [pl.BlockSpec(memory_space=pl.ANY)] * (len(inputs) - 3),
            out_specs=(pl.BlockSpec(memory_space=pltpu.VMEM),) * 3,
            scratch_shapes=[
                pltpu.VMEM((1, d), BF16),
                pltpu.VMEM((1, d), F32),
                pltpu.VMEM((1, LATENT), F32),
                pltpu.VMEM((1, d), F32),
                pltpu.VMEM((1, lanes), F32),
                pltpu.VMEM(cache_latent.shape[1:], BF16),
                pltpu.VMEM(cache_rope.shape[1:], BF16),
                pltpu.VMEM(w_absorb.shape, BF16),
                pltpu.VMEM(w_value.shape, BF16),
                pltpu.VMEM((feats, w_query.shape[1]), BF16),
                pltpu.VMEM((feats, w_latent.shape[1]), BF16),
                pltpu.VMEM((feats, w_rope.shape[1]), BF16),
                pltpu.VMEM((nm,) + w_output.shape, BF16),
                pltpu.VMEM((2, d, ff), BF16),
                pltpu.VMEM((2, d, ff), BF16),
                pltpu.VMEM((2, ff, d), BF16),
                pltpu.VMEM((nm, 1, feats), F32),
                pltpu.VMEM((nm, 1, feats), F32),
                pltpu.VMEM((6, 5, 1, feats), F32),
                pltpu.VMEM((6, 5, 1, feats), F32),
                pltpu.VMEM((nz, 1, lanes), F32),
                pltpu.VMEM((nm, 2, plain // 2), BF16),
                pltpu.VMEM((nm, 2, plain // 2), BF16),
                pltpu.VMEM((nm, 1, turned), F32),
                pltpu.VMEM((nm, 1, turned), F32),
                pltpu.VMEM((1, HEADS * VDIM), F32),
                pltpu.VMEM((4, 1, HEADS * VDIM), F32),
                pltpu.VMEM((4, 1, d), F32),
                pltpu.VMEM((4, 1, d), F32),
                pltpu.VMEM((2, d // 2), BF16),
                pltpu.VMEM((nz, 2, d // 2), BF16),
                pltpu.VMEM((nz, d), F32),
                pltpu.VMEM((nz, d), F32),
                pltpu.VMEM((nz, 2, d // 2), BF16),
                pltpu.VMEM((nz, 2, d // 2), BF16),
                dma((15,)),
                dma((nm,)),
                dma((nm,)),
                dma((nz,)),
                dma((nz,)),
                dma((6,)),
                dma((6,)),
                dma((nz,)),
                dma((nm,)),
                dma((nm,)),
                dma((nz,)),
                dma((nz,)),
                dma((9,)),
                dma((12,)),
                dma((3,)),
                dma((3,)),
                dma((nm // 2 * PIECES,)),
                dma((nm // 2 * PIECES,)),
                dma((nm // 2 * PIECES,)),
                dma((nm // 2 * PIECES,)),
                dma((nm * PIECES,)),
                dma((nm * PIECES,)),
                dma((7,)),
                dma((4,)),
                dma((4,)),
            ],
            compiler_params=pltpu.CompilerParams(
                collective_id=0, has_side_effects=True, vmem_limit_bytes=60 * 1024 * 1024
            ),
        )(*inputs)
        return pl.pallas_call(
            hand_over,
            out_shape=tuple(jax.ShapeDtypeStruct(o.shape, o.dtype) for o in outs),
            in_specs=[pl.BlockSpec(memory_space=pltpu.VMEM)] * 3,
            out_specs=(pl.BlockSpec(memory_space=pltpu.VMEM),) * 3,
        )(*outs)

    rows = P(("grp", "ep"), None)
    cached = P(("grp", "ep"), None, None)
    held = P("ep", None)
    experts = P("ep", None, None)
    return jax.shard_map(
        body,
        mesh=mesh,
        in_specs=(
            rows,
            cached,
            cached,
            P(("grp", "ep")),
            held,
            held,
            held,
            P(),
            P(),
            held,
            P(),
            P(),
            P(),
            rows,
            rows,
            experts,
            experts,
            experts,
        ),
        out_specs=(rows, rows, rows),
        check_vma=False,
    )
```

```python
import functools

import jax
import jax.numpy as jnp
import numpy as np
from jax import lax
from jax.experimental import pallas as pl
from jax.experimental.pallas import tpu as pltpu
from jax.sharding import PartitionSpec as P

HEADS = 16
NOPE = 64
ROPE = 32
VDIM = 64
LATENT = 512
EPS = 1e-06
THETA = 10000.0
MESH = pl.DeviceIdType.MESH
STEPS = (1, 3, 4)
DIGITS = (
    (0, 0, 0),
    (1, 0, 0),
    (-1, 1, 0),
    (0, 1, 0),
    (0, 0, 1),
    (1, 0, 1),
    (-1, 1, 1),
    (0, 1, 1),
    (1, 1, 1),
)
PIECES = 1
RING = (2, 4)
F32 = jnp.float32
BF16 = jnp.bfloat16


def rope_tables(position, lanes):
    place = lax.rem(lax.broadcasted_iota(jnp.int32, (1, lanes), 1), ROPE // 2)
    inverse = jnp.zeros((1, lanes), F32)
    for i in range(ROPE // 2):
        inverse = jnp.where(place == i, float(np.float32(THETA ** (-2.0 * i / ROPE))), inverse)
    angle = position.astype(F32) * inverse
    return (jnp.cos(angle), jnp.sin(angle))


def farthest_first(i, n):
    half = (i + 1) // 2
    return n // 2 + half * (1 - 2 * lax.rem(i, 2))


def rotate(x, cosine, sine):
    lanes = x.shape[-1]
    place = lax.rem(lax.broadcasted_iota(jnp.int32, x.shape, 1), ROPE)
    ahead = pltpu.roll(x, lanes - ROPE // 2, 1)
    behind = pltpu.roll(x, ROPE // 2, 1)
    return jnp.where(place < ROPE // 2, x * cosine - ahead * sine, x * cosine + behind * sine)


def dot(a, b):
    return jnp.dot(a, b, preferred_element_type=F32)


def dot_nt(a, b):
    return lax.dot_general(a, b, (((1,), (1,)), ((), ())), preferred_element_type=F32)


def kernel(
    nz,
    length_ref,
    routes_ref,
    scores_ref,
    tokens_hbm,
    cache_hbm,
    rope_hbm,
    wq_hbm,
    wl_hbm,
    wr_hbm,
    wa_hbm,
    wv_hbm,
    wo_hbm,
    gain_attn_hbm,
    gain_latent_hbm,
    gain_moe_hbm,
    wg_hbm,
    wu_hbm,
    wd_hbm,
    mixed_ref,
    new_latent_ref,
    new_rope_ref,
    tokens_v,
    gain_attn_v,
    gain_latent_v,
    gain_moe_v,
    wt_v,
    cache_v,
    rope_v,
    wa_v,
    wv_v,
    wq_v,
    wl_v,
    wr_v,
    wo_v,
    wg_v,
    wu_v,
    wd_v,
    p1_send,
    p1_recv,
    hop_send,
    hop_recv,
    wt_recv,
    p2_send,
    p2_recv,
    p2r_send,
    p2r_recv,
    v_send,
    v_recv,
    o_send,
    o_recv,
    p3_send,
    p3_recv,
    x3,
    c4,
    p4_send,
    p4_recv,
    local_sem,
    send16,
    send16r,
    send32,
    sendw,
    send_hop,
    recv_hop,
    wt_sem,
    p2_sem,
    p2r_sem,
    p3_sem,
    p4_sem,
    w_send,
    w_recv,
    e_send,
    e_recv,
    right_send,
    right_recv,
    left_send,
    left_recv,
    twin_send,
    twin_recv,
    quad_send,
    v_sem,
    o_sem,
):
    g = lax.axis_index("grp")
    q = lax.rem(g, 2)
    e = lax.axis_index("ep")
    z = e // 2
    c = lax.rem(e, 2)
    m = z // 2
    p = lax.rem(z, 2)
    nm = nz // 2
    ropes = wr_hbm.shape[1]
    fper = wq_hbm.shape[0]
    feats = 4 * fper
    d_model = tokens_hbm.shape[1]
    half = d_model // 2
    cache = cache_v.shape[0]

    def dev(zz, cc):
        return (g, zz * 2 + cc)

    beside = z + 1 - 2 * p
    right = lax.rem(z + 1, nz)
    left = lax.rem(z + nz - 1, nz)

    def remote(src, dst, send, recv, to):
        return pltpu.make_async_remote_copy(
            src_ref=src, dst_ref=dst, send_sem=send, recv_sem=recv, device_id=to, device_id_type=MESH
        )

    barrier = pltpu.get_barrier_semaphore()

    near = [dev(lax.rem(z + nz + k, nz), c) for k in (1, -1, 2, -2, 4, -4)]
    near += [dev(z, 1 - c), dev(beside, 1 - c), (g + 1 - 2 * q, e)]
    for device in near:
        pl.semaphore_signal(barrier, inc=1, device_id=device, device_id_type=MESH)

    block = 2 * p + c
    rows = pl.ds(pl.multiple_of(block * fper, fper), fper)
    loads = [
        (tokens_hbm, tokens_v),
        (gain_attn_hbm, gain_attn_v),
        (wq_hbm, wq_v.at[rows]),
        (wl_hbm, wl_v.at[rows]),
        (wr_hbm, wr_v.at[rows]),
        (gain_latent_hbm, gain_latent_v),
        (gain_moe_hbm, gain_moe_v),
        (wo_hbm, wo_v.at[m]),
        (wa_hbm, wa_v),
        (cache_hbm.at[0], cache_v),
        (rope_hbm.at[0], rope_v),
        (wv_hbm, wv_v),
        (wg_hbm.at[0], wg_v.at[c]),
        (wu_hbm.at[0], wu_v.at[c]),
        (wd_hbm.at[0], wd_v.at[c]),
    ]
    local = [pltpu.make_async_copy(a, b, local_sem.at[i]) for i, (a, b) in enumerate(loads)]
    for copy in local:
        copy.start()

    local[0].wait()
    local[1].wait()
    tokens = tokens_v[...].astype(F32)
    normed = tokens * lax.rsqrt(jnp.mean(tokens * tokens, axis=-1, keepdims=True) + EPS) * gain_attn_v[...]
    normed = normed.astype(BF16).astype(F32)
    blocks = [normed[:, i * feats : (i + 1) * feats] for i in range(nm)]
    for i in range(nm):
        p1_send[i] = blocks[i]
    p1_recv[m] = p1_send[m]
    pl.semaphore_wait(barrier, len(near))

    w_pairs = ((wq_hbm, wq_v), (wl_hbm, wl_v), (wr_hbm, wr_v))
    w_targets = (dev(beside, c), dev(z, 1 - c))
    across = 2 * (1 - p) + c

    def w_copies(slot, k):
        at = pl.ds(pl.multiple_of(slot * fper, fper), fper)
        return [
            remote(
                src if k < 2 else dst.at[at],
                dst.at[at],
                w_send.at[3 * k + j],
                w_recv.at[3 * slot + j],
                w_targets[min(k, 1)],
            )
            for j, (src, dst) in enumerate(w_pairs)
        ]

    piece = half // PIECES

    def member(k):
        return lax.rem(m + nm + k, nm)

    def to_class(k):
        return dev(2 * member(k) + p, c)

    def lanes_of(which, k):
        return pl.ds(pl.multiple_of(which * half + k * piece, piece), piece)

    def wo_piece(mm, k):
        return wo_v.at[mm, :, lanes_of(q, k)]

    def to_twin(mm, k, which):
        part = wo_v.at[mm, :, lanes_of(which, k)]
        i = mm * PIECES + k
        return remote(part, part, twin_send.at[i], twin_recv.at[i], (g + 1 - 2 * q, e))

    def to_right(mm, s, k, src=None):
        i = s * PIECES + k
        dst = wo_piece(mm, k)
        return remote(dst if src is None else src, dst, right_send.at[i], right_recv.at[i], to_class(1))

    def to_left(mm, s, k, src=None):
        i = s * PIECES + k
        dst = wo_piece(mm, k)
        return remote(dst if src is None else src, dst, left_send.at[i], left_recv.at[i], to_class(-1))

    def ring_start():
        for k in range(PIECES):
            own = wo_hbm.at[:, lanes_of(q, k)]
            to_right(m, 0, k, own).start()
            to_left(m, 0, k, own).start()

    def ring_step(s, leftward, pass_right, pass_left):
        from_left = member(-s)
        from_right = member(s)
        for k in range(PIECES):
            to_right(from_left, s - 1, k).wait_recv()
            if pass_right:
                to_right(from_left, s, k).start()
            to_twin(from_left, k, q).start()
            if leftward:
                to_left(from_right, s - 1, k).wait_recv()
                if pass_left:
                    to_left(from_right, s, k).start()
                to_twin(from_right, k, q).start()

    def ring(first, last):
        for s in range(first, last + 1):
            ring_step(s, s < nm // 2, s < nm // 2, s < nm // 2 - 1)

    e_pairs = ((wg_hbm, wg_v), (wu_hbm, wu_v), (wd_hbm, wd_v))

    def e_copies(slot):
        return [
            remote(src.at[0], dst.at[slot], e_send.at[j], e_recv.at[j], dev(z, 1 - c))
            for j, (src, dst) in enumerate(e_pairs)
        ]

    digits = {o: DIGITS[abs(o)] if o >= 0 else tuple(-x for x in DIGITS[-o]) for o in range(1 - nm // 2, nm // 2 + 1)}
    place = {}
    for r in range(len(STEPS)):
        for sign in (1, -1):
            at = [o for o in digits if digits[o][r] == sign]
            for i, o in enumerate(at):
                place[o, r] = i

    def p1_round(r, sign):
        count = sum(1 for o in digits if digits[o][r] == sign)
        to = 2 * member(sign * STEPS[r]) + p
        i = 2 * r + (sign < 0)
        part = pl.ds(0, count)
        return remote(hop_send.at[i, part], hop_recv.at[i, part], send_hop.at[i], recv_hop.at[i], dev(to, c))

    def last_hop(o, r):
        for earlier in range(r - 1, -1, -1):
            if digits[o][earlier]:
                return earlier
        return None

    def p1_start(r):
        for o in digits:
            if digits[o][r]:
                held = last_hop(o, r)
                if held is None:
                    block_o = p1_send[member(o)]
                else:
                    block_o = hop_recv[2 * held + (digits[o][held] < 0), place[o, held]]
                hop_send[2 * r + (digits[o][r] < 0), place[o, r]] = block_o
        p1_round(r, 1).start()
        p1_round(r, -1).start()

    def p1_wait(r):
        p1_round(r, 1).wait_recv()
        p1_round(r, -1).wait_recv()

    p1_start(0)
    for k in range(2):
        for copy in w_copies(block, k):
            copy.start()
    ring_start()
    for copy in e_copies(c):
        copy.start()
    lane = lax.broadcasted_iota(jnp.int32, wt_v.shape, 1)
    first = jnp.full(wt_v.shape, scores_ref[0, 0], F32)
    second = jnp.full(wt_v.shape, scores_ref[0, 1], F32)
    both = first + second
    wt_v[...] = jnp.where(lane == routes_ref[0, 0], first / both, 0.0) + jnp.where(
        lane == routes_ref[0, 1], second / both, 0.0
    )
    wt_recv[z] = wt_v[...]
    cosine, sine = rope_tables(length_ref[0], HEADS * ROPE)
    p2r_send[...] = jnp.zeros_like(p2r_send)
    p1_wait(0)
    p1_start(1)
    for here, there in zip(w_copies(across, 0), w_copies(across, 2)):
        here.wait_recv()
        there.start()
    ring(1, RING[0])
    p1_wait(1)
    p1_start(2)
    ring(RING[0] + 1, RING[1])

    for copy in local[2:5]:
        copy.wait()
    for slot in (2 * p + 1 - c, 2 * (1 - p) + 1 - c):
        for copy in w_copies(slot, 1):
            copy.wait_recv()
    p1_wait(2)
    for o in digits:
        if o:
            held = last_hop(o, len(STEPS))
            p1_recv[member(-o)] = hop_recv[2 * held + (digits[o][held] < 0), place[o, held]]

    x1 = p1_recv[:, 0, :].astype(BF16)
    part_q = dot(x1, wq_v[...])
    part_l = dot(x1, wl_v[...])
    part_r = dot(x1, wr_v[...])
    size = NOPE + ROPE
    nope, turned = HEADS * NOPE, HEADS * ROPE
    part_n = jnp.concatenate([part_q[:, h * size : h * size + NOPE] for h in range(HEADS)], axis=1)
    part_p = jnp.concatenate([part_q[:, h * size + NOPE : (h + 1) * size] for h in range(HEADS)], axis=1)
    plain = jnp.concatenate([part_n, part_l], axis=1)
    fold2 = plain.shape[1] // 2
    for i in range(nm):
        row = plain[i : i + 1, :]
        p2_send[i] = jnp.concatenate([row[:, :fold2], row[:, fold2:]], axis=0).astype(BF16)
        p2r_send[i, :, 0:turned] = part_p[i : i + 1, :]
        p2r_send[i, :, turned : turned + ropes] = part_r[i : i + 1, :]

    def p2_copy(to, slot, d):
        return remote(p2_send.at[to], p2_recv.at[slot], send16.at[d], p2_sem.at[slot], dev(2 * to + p, c))

    def p2r_copy(to, slot, d):
        return remote(p2r_send.at[to], p2r_recv.at[slot], send16r.at[d], p2r_sem.at[slot], dev(2 * to + p, c))

    def p2_start(i, _):
        d = farthest_first(i, nm)
        to = lax.rem(m + d, nm)
        p2r_copy(to, m, d).start()
        p2_copy(to, m, d).start()
        return 0

    lax.fori_loop(0, nm - 1, p2_start, 0)

    ring(RING[1] + 1, nm // 2 - 2)

    def p2_wait(i, acc):
        d = nm - 1 - i
        src = lax.rem(m + nm - d, nm)
        p2r_copy(m, src, d).wait_recv()
        p2_copy(m, src, d).wait_recv()
        return (acc[0] + p2_recv[src].astype(F32), acc[1] + p2r_recv[src])

    folded, turns = lax.fori_loop(0, nm - 1, p2_wait, (p2_send[m].astype(F32), p2r_send[m]))
    summed = jnp.concatenate([folded[0:1], folded[1:2]], axis=1)

    for copy in local[5:7]:
        copy.wait()
    q_nope = summed[:, :nope].astype(BF16).astype(F32)
    q_rope = turns[:, :turned].astype(BF16).astype(F32)
    latent_raw = summed[:, nope:].astype(BF16).astype(F32)
    rope_raw = turns[:, turned:].astype(BF16).astype(F32)
    new_latent = (
        latent_raw
        * lax.rsqrt(jnp.mean(latent_raw * latent_raw, axis=-1, keepdims=True) + EPS)
        * gain_latent_v[...]
    ).astype(BF16)
    new_rope = rotate(rope_raw, cosine[:, : rope_raw.shape[1]], sine[:, : rope_raw.shape[1]]).astype(BF16)
    new_latent_ref[...] = new_latent
    new_rope_ref[...] = new_rope[:, :ropes]

    q_rope = rotate(q_rope, cosine, sine).astype(BF16).astype(F32)

    def by_head(row, width):
        shape = (HEADS, row.shape[1])
        own = lax.broadcasted_iota(jnp.int32, shape, 1) // width == lax.broadcasted_iota(jnp.int32, shape, 0)
        return jnp.where(own, jnp.broadcast_to(row, shape), 0.0)

    fold_shape = (HEADS * ROPE, ROPE)
    fold = (
        lax.rem(lax.broadcasted_iota(jnp.int32, fold_shape, 0), ROPE)
        == lax.broadcasted_iota(jnp.int32, fold_shape, 1)
    ).astype(F32).astype(BF16)
    q_pe = dot(by_head(q_rope, ROPE).astype(BF16), fold).astype(BF16)
    local[8].wait()
    q_abs = dot_nt(by_head(q_nope, NOPE).astype(BF16), wa_v[...]).astype(BF16)

    ring(nm // 2 - 1, nm // 2 - 1)
    local[9].wait()
    local[10].wait()
    scale = (NOPE + ROPE) ** (-0.5)
    past = (dot_nt(q_abs, cache_v[...]) + dot(q_pe, rope_v[...])) * scale
    fresh = (
        jnp.sum(q_abs.astype(F32) * new_latent.astype(F32), axis=-1, keepdims=True)
        + jnp.sum(q_pe.astype(F32) * new_rope[:, :ropes].astype(F32), axis=-1, keepdims=True)
    ) * scale
    valid = lax.broadcasted_iota(jnp.int32, past.shape, 1) < length_ref[0]
    top = jnp.maximum(jnp.max(jnp.where(valid, past, -jnp.inf), axis=-1, keepdims=True), fresh)
    e_past = jnp.where(valid, jnp.exp(past - top), 0.0)
    e_new = jnp.exp(fresh - top)
    total = jnp.sum(e_past, axis=-1, keepdims=True) + e_new
    p_past = (e_past / total).astype(BF16)
    p_new = (e_new / total).astype(BF16).astype(F32)
    attended = (dot(p_past, cache_v[...]) + p_new * new_latent.astype(F32)).astype(BF16)
    local[11].wait()
    crossed = dot(attended, wv_v[...])
    own_head = (
        lax.broadcasted_iota(jnp.int32, crossed.shape, 1) // VDIM
        == lax.broadcasted_iota(jnp.int32, crossed.shape, 0)
    )
    values = jnp.sum(jnp.where(own_head, crossed, 0.0), axis=0, keepdims=True).astype(BF16)

    def beside_me(slot):
        return dev(z - p + slot // 2, lax.rem(slot, 2))

    def v_copy(slot, k):
        return remote(v_send, v_recv.at[slot], quad_send.at[k], v_sem.at[slot], beside_me(lax.rem(block + k, 4)))

    def o_copy(to, slot, k):
        return remote(o_send.at[to], o_recv.at[slot], quad_send.at[3 + k], o_sem.at[slot], beside_me(to))

    v_send[...] = values.astype(F32)
    for k in range(1, 4):
        v_copy(block, k).start()
    v_recv[block] = v_send[...]
    ring(nm // 2, nm // 2)

    vals, own_rows = HEADS * VDIM, nm * wo_hbm.shape[0]
    vper = wo_hbm.shape[0]
    at = lax.broadcasted_iota(jnp.int32, (vals, own_rows), 0)
    row = lax.broadcasted_iota(jnp.int32, (vals, own_rows), 1)
    pick = (at == (4 * (row // vper) + block) * vper + lax.rem(row, vper)).astype(F32).astype(BF16)
    local[7].wait()
    for i in range(1, nm):
        for k in range(PIECES):
            to_twin(member(i), k, 1 - q).wait_recv()
    for k in range(1, 4):
        v_copy(lax.rem(block + k, 4), k).wait_recv()
    picked = dot(v_recv[:, 0, :].astype(BF16), pick).astype(BF16)
    part_o = dot(picked, wo_v[...].reshape(own_rows, d_model))
    for i in range(4):
        o_send[i] = part_o[i : i + 1, :]
    for k in range(1, 4):
        o_copy(lax.rem(block + k, 4), block, k).start()

    def wt_copy(to, slot, d):
        return remote(wt_v, wt_recv.at[slot], sendw.at[d], wt_sem.at[slot], dev(to, c))

    def wt_start(i, _):
        d = farthest_first(i, nz)
        wt_copy(lax.rem(z + d, nz), z, d).start()
        return 0

    lax.fori_loop(0, nz - 1, wt_start, 0)

    attn_out = o_send[block]
    for k in range(1, 4):
        slot = lax.rem(block + k, 4)
        o_copy(block, slot, k).wait_recv()
        attn_out = attn_out + o_recv[slot]
    resid = (tokens + attn_out).astype(BF16).astype(F32)
    moe_in = resid * lax.rsqrt(jnp.mean(resid * resid, axis=-1, keepdims=True) + EPS) * gain_moe_v[...]
    moe_in = moe_in.astype(BF16).astype(F32)
    p3_send[...] = jnp.concatenate([moe_in[:, :half], moe_in[:, half:]], axis=0).astype(BF16)

    def p3_copy(to, slot, d):
        return remote(p3_send, p3_recv.at[slot], send32.at[d], p3_sem.at[slot], dev(to, c))

    def p3_start(i, _):
        d = farthest_first(i, nz)
        p3_copy(lax.rem(z + d, nz), z, d).start()
        return 0

    lax.fori_loop(0, nz - 1, p3_start, 0)
    x3[pl.ds(z, 1), :] = moe_in

    for copy in local[12:15]:
        copy.wait()
    for copy in e_copies(1 - c):
        copy.wait_recv()

    def wt_wait(i, _):
        d = i + 1
        wt_copy(z, lax.rem(z + nz - d, nz), d).wait()
        return 0

    lax.fori_loop(0, nz - 1, wt_wait, 0)

    def p3_wait(i, _):
        near = i // 2 + 1
        src = lax.rem(z + nz + near * (1 - 2 * lax.rem(i, 2)), nz)
        p3_copy(z, src, 0).wait_recv()
        row = p3_recv[src].astype(F32)
        x3[pl.ds(src, 1), 0:half] = row[0:1]
        x3[pl.ds(src, 1), half:d_model] = row[1:2]
        return 0

    lax.fori_loop(0, nz - 1, p3_wait, 0)

    def p3_sent(d, _):
        p3_copy(z, z, d).wait_send()
        return 0

    lax.fori_loop(1, nz, p3_sent, 0)

    rows3 = x3[...].astype(BF16)
    shares = wt_recv[:, 0, :]
    expert = lax.broadcasted_iota(jnp.int32, shares.shape, 1)
    outs = []
    for s in range(2):
        share = jnp.sum(jnp.where(expert == 2 * z + s, shares, 0.0), axis=1, keepdims=True)
        gate = dot(rows3, wg_v[s])
        upper = dot(rows3, wu_v[s])
        hidden = (jax.nn.silu(gate) * upper).astype(BF16)
        result = dot(hidden, wd_v[s]).astype(BF16).astype(F32)
        outs.append(share * result)
    c4[...] = outs[0] + outs[1]

    def p4_copy(to, slot, d):
        return remote(p4_send.at[to], p4_recv.at[slot], send32.at[d], p4_sem.at[slot], dev(to, c))

    def p4_start(i, _):
        d = farthest_first(i, nz)
        to = lax.rem(z + d, nz)
        row = c4[pl.ds(to, 1), :]
        p4_send[to] = jnp.concatenate([row[:, :half], row[:, half:]], axis=0).astype(BF16)
        p4_copy(to, z, d).start()
        return 0

    lax.fori_loop(0, nz - 1, p4_start, 0)
    mine = c4[pl.ds(z, 1), :]

    def p4_wait(i, acc):
        near = i // 2 + 1
        src = lax.rem(z + nz + near * (1 - 2 * lax.rem(i, 2)), nz)
        p4_copy(z, src, 0).wait_recv()
        return acc + p4_recv[src].astype(F32)

    acc = lax.fori_loop(
        0, nz - 1, p4_wait, jnp.concatenate([mine[:, :half], mine[:, half:]], axis=0)
    )
    mixed_ref[:, :half] = (resid[:, :half] + acc[0:1]).astype(BF16)
    mixed_ref[:, half:] = (resid[:, half:] + acc[1:2]).astype(BF16)

    def p4_sent(d, _):
        p4_copy(z, z, d).wait_send()
        return 0

    lax.fori_loop(1, nz, p4_sent, 0)

    def p2_sent(d, _):
        p2_copy(m, m, d).wait_send()
        p2r_copy(m, m, d).wait_send()
        return 0

    lax.fori_loop(1, nm, p2_sent, 0)
    for k in range(2):
        for copy in w_copies(block, k):
            copy.wait_send()
    for copy in w_copies(across, 2):
        copy.wait_send()
    for copy in e_copies(c):
        copy.wait_send()

    for i in range(nm // 2):
        for k in range(PIECES):
            to_right(m, i, k).wait_send()
            if i < nm // 2 - 1:
                to_left(m, i, k).wait_send()
    for i in range(1, nm):
        for k in range(PIECES):
            to_twin(member(i), k, q).wait_send()
    for k in range(1, 4):
        v_copy(block, k).wait_send()
        o_copy(block, block, k).wait_send()
    for r in range(len(STEPS)):
        p1_round(r, 1).wait_send()
        p1_round(r, -1).wait_send()


def hand_over(a, b, c, x, y, w):
    x[...] = a[...]
    y[...] = b[...]
    w[...] = c[...]


def solution(mesh):
    n = mesh.shape["ep"]
    nz = n // 2
    nm = nz // 2

    def body(
        tokens,
        cache_latent,
        cache_rope,
        lengths,
        w_query,
        w_latent,
        w_rope,
        w_absorb,
        w_value,
        w_output,
        gain_attn,
        gain_latent,
        gain_moe,
        routes,
        route_scores,
        w_gate,
        w_up,
        w_down,
    ):
        d = tokens.shape[1]
        lanes = max(128, n)
        fper = w_query.shape[0]
        feats = 4 * fper
        plain = HEADS * NOPE + w_latent.shape[1]
        turned = HEADS * ROPE + 128
        ff = w_gate.shape[2]
        inputs = (
            lengths,
            routes,
            route_scores,
            tokens,
            cache_latent,
            cache_rope,
            w_query,
            w_latent,
            w_rope,
            w_absorb,
            w_value,
            w_output,
            gain_attn[None, :],
            gain_latent[None, :],
            gain_moe[None, :],
            w_gate,
            w_up,
            w_down,
        )
        dma = pltpu.SemaphoreType.DMA
        outs = pl.pallas_call(
            functools.partial(kernel, nz),
            out_shape=(
                jax.ShapeDtypeStruct((1, d), BF16),
                jax.ShapeDtypeStruct((1, LATENT), BF16),
                jax.ShapeDtypeStruct((1, ROPE), BF16),
            ),
            in_specs=[pl.BlockSpec(memory_space=pltpu.SMEM)] * 3
            + [pl.BlockSpec(memory_space=pl.ANY)] * (len(inputs) - 3),
            out_specs=(pl.BlockSpec(memory_space=pltpu.VMEM),) * 3,
            scratch_shapes=[
                pltpu.VMEM((1, d), BF16),
                pltpu.VMEM((1, d), F32),
                pltpu.VMEM((1, LATENT), F32),
                pltpu.VMEM((1, d), F32),
                pltpu.VMEM((1, lanes), F32),
                pltpu.VMEM(cache_latent.shape[1:], BF16),
                pltpu.VMEM(cache_rope.shape[1:], BF16),
                pltpu.VMEM(w_absorb.shape, BF16),
                pltpu.VMEM(w_value.shape, BF16),
                pltpu.VMEM((feats, w_query.shape[1]), BF16),
                pltpu.VMEM((feats, w_latent.shape[1]), BF16),
                pltpu.VMEM((feats, w_rope.shape[1]), BF16),
                pltpu.VMEM((nm,) + w_output.shape, BF16),
                pltpu.VMEM((2, d, ff), BF16),
                pltpu.VMEM((2, d, ff), BF16),
                pltpu.VMEM((2, ff, d), BF16),
                pltpu.VMEM((nm, 1, feats), F32),
                pltpu.VMEM((nm, 1, feats), F32),
                pltpu.VMEM((6, 5, 1, feats), F32),
                pltpu.VMEM((6, 5, 1, feats), F32),
                pltpu.VMEM((nz, 1, lanes), F32),
                pltpu.VMEM((nm, 2, plain // 2), BF16),
                pltpu.VMEM((nm, 2, plain // 2), BF16),
                pltpu.VMEM((nm, 1, turned), F32),
                pltpu.VMEM((nm, 1, turned), F32),
                pltpu.VMEM((1, HEADS * VDIM), F32),
                pltpu.VMEM((4, 1, HEADS * VDIM), F32),
                pltpu.VMEM((4, 1, d), F32),
                pltpu.VMEM((4, 1, d), F32),
                pltpu.VMEM((2, d // 2), BF16),
                pltpu.VMEM((nz, 2, d // 2), BF16),
                pltpu.VMEM((nz, d), F32),
                pltpu.VMEM((nz, d), F32),
                pltpu.VMEM((nz, 2, d // 2), BF16),
                pltpu.VMEM((nz, 2, d // 2), BF16),
                dma((15,)),
                dma((nm,)),
                dma((nm,)),
                dma((nz,)),
                dma((nz,)),
                dma((6,)),
                dma((6,)),
                dma((nz,)),
                dma((nm,)),
                dma((nm,)),
                dma((nz,)),
                dma((nz,)),
                dma((9,)),
                dma((12,)),
                dma((3,)),
                dma((3,)),
                dma((nm // 2 * PIECES,)),
                dma((nm // 2 * PIECES,)),
                dma((nm // 2 * PIECES,)),
                dma((nm // 2 * PIECES,)),
                dma((nm * PIECES,)),
                dma((nm * PIECES,)),
                dma((7,)),
                dma((4,)),
                dma((4,)),
            ],
            compiler_params=pltpu.CompilerParams(
                collective_id=0, has_side_effects=True, vmem_limit_bytes=60 * 1024 * 1024
            ),
        )(*inputs)
        return pl.pallas_call(
            hand_over,
            out_shape=tuple(jax.ShapeDtypeStruct(o.shape, o.dtype) for o in outs),
            in_specs=[pl.BlockSpec(memory_space=pltpu.VMEM)] * 3,
            out_specs=(pl.BlockSpec(memory_space=pltpu.VMEM),) * 3,
        )(*outs)

    rows = P(("grp", "ep"), None)
    cached = P(("grp", "ep"), None, None)
    held = P("ep", None)
    experts = P("ep", None, None)
    return jax.shard_map(
        body,
        mesh=mesh,
        in_specs=(
            rows,
            cached,
            cached,
            P(("grp", "ep")),
            held,
            held,
            held,
            P(),
            P(),
            held,
            P(),
            P(),
            P(),
            rows,
            rows,
            experts,
            experts,
            experts,
        ),
        out_specs=(rows, rows, rows),
        check_vma=False,
    )
```
